512 devices in a mesh: sp: 32 (over z, core), tp: 16 (over y, x).
Axes of the slice: x: 4, y: 4, z: 16, core: 2. Of those that a mesh axis runs over, the one named last changes fastest.
Arguments:
- out_gate: bfloat16 [8192, 512], P('sp', 'tp'), may hold values from -6 to 6
- in_gate: bfloat16 [8192, 512], P('sp', 'tp'), may hold values from -6 to 6
- conv_input: bfloat16 [8192, 512], P('sp', 'tp'), may hold values from -6 to 6
- conv_taps: float32 [3, 512], P(None, 'tp'), may hold values from -3.5 to 3.5
- out_weight: bfloat16 [512, 2048], P('tp'), may hold values from -0.25 to 0.25
- residual: bfloat16 [8192, 2048], P('sp', 'tp'), may hold values from -60 to 60
- document: int32 [8192], P('sp'), may hold values from 0 to 7, never falling along the last dimension, each value on 1 to 2048 neighbouring positions
- mix_gain: float32 [2048], P('tp'), may hold values from 0.15 to 3
- ffn_gain: float32 [2048], P('tp'), may hold values from 0.1 to 1.9
- routes: int32 [8192, 2], P('sp'), may hold values from 0 to 31, all different within a row; in each aligned block of 256 rows (0 to 255, 256 to 511, ...) at most 32 rows name the same one
- route_weight: float32 [8192, 2], P('sp'), may hold values from 0.1 to 1
- expert_gate: bfloat16 [32, 2048, 4096], P('sp', None, 'tp'), may hold values from -0.375 to 0.375
- expert_up: bfloat16 [32, 2048, 4096], P('sp', None, 'tp'), may hold values from -0.375 to 0.375
- expert_down: bfloat16 [32, 4096, 2048], P('sp', None, 'tp'), may hold values from -0.09375 to 0.09375
Outputs:
- result: bfloat16 [8192, 2048], P('sp', 'tp')
The draws below stay inside these ranges and needn't reach their ends.
Inputs may be any that keep to these rules, and one draw needn't show every extreme that they name: `routes`: within each aligned block of 256 rows, no expert is named more than 32 times; some expert is named exactly 32 times in some blocks. The 2 experts of a row differ. Document numbers never fall along the positions; each document is one contiguous run.
All inputs are finite; a program needn't handle non-finite values.
Results may differ from the reference program's by a relative error of at most 0.0069.
Values may be sent and summed in bfloat16 or wider, within the bound.
A program may use at most 64 MiB of HBM per device.

```python
import math
import jax
import jax.numpy as jnp
import numpy as np
from jax import lax

D = 2048
CONV = 512
FF = 4096
TOPK = 2
TAPS = 3
TOK = 256
TOKENS = 8192
EXPERTS = 32
CAP = 32
N_SP = 32


def draw_residual(key, part):
    noise_key, column_key = jax.random.split(jax.random.fold_in(key, 11), 2)
    columns = jnp.arange(D, dtype=jnp.float32) / D
    rising = jnp.exp(jnp.log(3.0) * columns)
    scatter = jnp.exp(jax.random.uniform(column_key, (D,), jnp.float32, jnp.log(0.5), jnp.log(2.0)))
    values = jnp.clip(jax.random.normal(noise_key, (TOKENS, D), jnp.float32), -6.0, 6.0)
    return (values * rising[None, :] * scatter[None, :] * 0.6).astype(jnp.bfloat16)


def draw_mix_gain(key, part):
    columns = jnp.arange(D, dtype=jnp.float32) / D
    rising = jnp.exp(jnp.log(3.0) * (columns - 0.5))
    gain_key = jax.random.fold_in(key, 23)
    wobble = jax.random.uniform(gain_key, (D,), jnp.float32, 0.5, 1.5)
    return rising * wobble


def level_of(rng, shape, cuts, low, largest):
    factor_of, own = 1.0, jax.random.fold_in(rng, 6)
    for dim, blocks in cuts:
        draws = jnp.exp(jax.random.uniform(jax.random.fold_in(own, dim), (blocks,), jnp.float32, low / len(cuts), largest / len(cuts)))
        factor_of = factor_of * jnp.repeat(draws, shape[dim] // blocks).reshape([-1 if axis == dim else 1 for axis in range(len(shape))])
    return factor_of


def length_profile(amount, total, reach, slope):
    loads = [(1 << 20) // math.isqrt(grade ** slope) + 1 for grade in range(2, amount + 1)]
    spare, given = total - reach - (amount - 1), [1] * (amount - 1)
    while spare > 0:
        movable = [i for i in range(amount - 1) if given[i] < reach]
        whole, remaining = sum([loads[i] for i in movable]), spare
        for i in movable:
            extra = min(reach - given[i], max(1, remaining * loads[i] // whole), spare)
            given[i] = given[i] + extra
            spare = spare - extra
    return np.array([reach] + given)


def ragged_sizes(key, count, total, reach, skew):
    if count == 2:
        one = jax.random.randint(key, (), max(1, total - reach), min(reach, total - 1) + 1)
        return jnp.stack([one, total - one])
    lengths = jnp.asarray(length_profile(count, total, reach, skew), jnp.int32)
    twos = (count - 1) // 2
    giver, receiver = lengths[1:1 + 2 * twos:2], lengths[2:2 + 2 * twos:2]
    slack = jnp.minimum(giver - 1, reach - receiver)
    passed = jax.random.randint(jax.random.fold_in(key, 1), (twos,), 0, 1 << 20) % (slack + 1)
    lengths = lengths.at[1:1 + 2 * twos:2].set(giver - passed).at[2:2 + 2 * twos:2].set(receiver + passed)
    return lengths[jax.random.permutation(jax.random.fold_in(key, 2), count)]


def assign_block(stream_key, own, number, rows, count, top, limit, skew):
    sequence = jax.random.permutation(stream_key, count)
    heavy_load, ordinary = load_shares(count, rows * top, limit, skew, True), load_shares(count, rows * top, limit, skew, False)
    places = jnp.arange(count)

    def named(tallies, offset_by):
        used = int((tallies > 0).sum())
        fixed = max(1, used // 4)
        shifted = fixed + (places - fixed + offset_by * (used - fixed)) % max(1, count - fixed)
        return jnp.zeros((count,), jnp.int32).at[sequence[jnp.where(places < fixed, places, shifted)]].set(jnp.asarray(tallies, jnp.int32))

    tallies = jnp.where(number % 4 == 0, named(heavy_load, number // 4), named(ordinary, number - number // 4 - 1))
    mixed = jax.random.permutation(jax.random.fold_in(own, 3), count)
    giver, receiver = mixed[0:count // 2 * 2:2], mixed[1:count // 2 * 2:2]
    margin = jnp.minimum(tallies[giver] - 1, limit - tallies[receiver]) // 2
    margin = jnp.where((giver == sequence[0]) | (receiver == sequence[0]) | (tallies[receiver] == 0), 0, jnp.maximum(margin, 0))
    shifted = jax.random.randint(jax.random.fold_in(own, 4), (count // 2,), 0, 1 << 20) % (margin + 1)
    tallies = tallies.at[giver].add(-shifted).at[receiver].add(shifted)
    items = jnp.searchsorted(jnp.cumsum(tallies), jnp.arange(rows * top), side="right").astype(jnp.int32)
    listing = items.reshape(top, rows).T
    listing = listing[jax.random.permutation(jax.random.fold_in(own, 1), rows)]
    offset_by = jax.random.randint(jax.random.fold_in(own, 2), (rows, 1), 0, top)
    return jnp.take_along_axis(listing, (jnp.arange(top)[None, :] + offset_by) % top, axis=1)


def load_shares(number_of, total, limit, slope, full):
    weights = [(1 << 20) // math.isqrt(grade ** slope) + 1 for grade in range(1, number_of + 1)]
    largest = limit if full else min(limit, max(-(-total // number_of), total * weights[0] // sum(weights)))
    least = 1 if total - largest >= number_of - 1 else 0
    holding, spare = [largest] + [least] * (number_of - 1), total - largest - least * (number_of - 1)
    while spare > 0:
        free = [i for i in range(1, number_of) if holding[i] < largest] or [i for i in range(1, number_of) if holding[i] < limit]
        whole, left = sum([weights[i] for i in free]), spare
        for i in free:
            extra = min(limit - holding[i], max(1, left * weights[i] // whole), spare)
            holding[i] = holding[i] + extra
            spare = spare - extra
    return np.array(holding)


def centred(key, extent, scale, bound, cuts=(), kind=jnp.bfloat16):
    values = jax.random.normal(key, extent, jnp.float32) * scale
    if len(cuts) > 0:
        values = level_of(key, extent, cuts, -0.22, 0.18) * values
    return jnp.clip(values, min=-bound, max=bound).astype(kind)


def setup_inputs(seed: int = 0) -> dict:
    seeds = jax.random.split(jax.random.key(seed), 15)
    out_gate = centred(seeds[0], (TOKENS, CONV), 1.0, 6.0, ((0, 32), (1, 16)))
    in_gate = centred(seeds[1], (TOKENS, CONV), 1.0, 6.0, ((0, 32), (1, 16)))
    conv_input = centred(seeds[2], (TOKENS, CONV), 1.0, 6.0, ((0, 32), (1, 16)))
    conv_taps = centred(seeds[3], (TAPS, CONV), TAPS ** -0.5, 3.5, ((1, 16),), jnp.float32)
    out_weight = centred(seeds[4], (CONV, D), CONV ** -0.5, 0.25, ((0, 16),))
    residual = draw_residual(jax.random.fold_in(seeds[14], 71), 0)
    document = jnp.searchsorted(jnp.cumsum(ragged_sizes(seeds[6], max(2, N_SP // 4), TOKENS, 2 * TOKENS // max(2, N_SP // 4), 0)), jnp.arange(TOKENS), side="right").astype(jnp.int32)
    mix_gain = draw_mix_gain(jax.random.fold_in(seeds[14], 71), 0)
    ffn_gain = jnp.clip(1.0 + 0.18 * jax.random.normal(seeds[8], (D,), jnp.float32), 0.1, 1.9)
    routes_keys = jax.random.split(jax.random.fold_in(seeds[9], 1), TOKENS // TOK)
    routes_turns = jax.random.permutation(jax.random.fold_in(seeds[9], 3), TOKENS // TOK)
    routes = jax.vmap(lambda own, number: assign_block(jax.random.fold_in(seeds[9], 2), own, number, TOK, EXPERTS, TOPK, CAP, 1))(routes_keys, routes_turns).reshape((TOKENS, TOPK))
    route_weight = jnp.clip(0.1 + 0.9 * jax.random.uniform(seeds[10], (TOKENS, TOPK), jnp.float32) ** level_of(seeds[10], (TOKENS, TOPK), ((0, 32),), -0.2, 0.2), 0.1, 1.0)
    expert_gate = centred(seeds[11], (EXPERTS, D, FF), (D // 8) ** -0.5, 0.375, ((0, 32), (2, 16)))
    expert_up = centred(seeds[12], (EXPERTS, D, FF), (D // 8) ** -0.5, 0.375, ((0, 32), (2, 16)))
    expert_down = centred(seeds[13], (EXPERTS, FF, D), FF ** -0.5, 0.09375, ((0, 32), (2, 16)))
    return {"out_gate": out_gate, "in_gate": in_gate, "conv_input": conv_input, "conv_taps": conv_taps, "out_weight": out_weight, "residual": residual, "document": document, "mix_gain": mix_gain, "ffn_gain": ffn_gain, "routes": routes, "route_weight": route_weight, "expert_gate": expert_gate, "expert_up": expert_up, "expert_down": expert_down}


ALPHA = 8.0 ** 0.25
EPSILON = 1e-05
LIMIT = 7.0
SLOPE = 1.702

def layer_norm(stream, gain_row):
    row_mean = lax.optimization_barrier(jnp.sum(stream, axis=1)) / D
    row_spread = lax.optimization_barrier(jnp.sum(stream * stream, axis=1)) / D - row_mean * row_mean
    scaled = (stream - row_mean[:, None]) * lax.rsqrt(row_spread + EPSILON)[:, None]
    return (scaled * gain_row[None, :]).astype(jnp.bfloat16)

def clamped_unit(gate_pre, up_pre):
    gate_part = jnp.minimum(gate_pre, LIMIT)
    up_part = jnp.clip(up_pre, -LIMIT, LIMIT)
    return ((up_part + 1.0) * gate_part * jax.nn.sigmoid(SLOPE * gate_part)).astype(jnp.bfloat16)

def reference(out_gate, in_gate, conv_input, conv_taps, out_weight, residual, document, mix_gain, ffn_gain, routes, route_weight, expert_gate, expert_up, expert_down):
    product = in_gate.astype(jnp.float32) * conv_input.astype(jnp.float32)
    padded = jnp.concatenate([jnp.zeros((2, CONV), jnp.float32), product], axis=0)
    doc_marks = jnp.concatenate([jnp.full((2,), -1, jnp.int32), document.astype(jnp.int32)], axis=0)
    same_one = (doc_marks[1:-1] == document).astype(jnp.float32)[:, None]
    same_two = (doc_marks[:-2] == document).astype(jnp.float32)[:, None]
    mixed_rows = conv_taps[2][None, :] * product + same_one * conv_taps[1][None, :] * padded[1:-1] + same_two * conv_taps[0][None, :] * padded[:-2]
    conv_out = (out_gate.astype(jnp.float32) * mixed_rows).astype(jnp.bfloat16)
    mixer_sum = jnp.dot(conv_out, out_weight, preferred_element_type=jnp.float32)
    normed = layer_norm(ALPHA * residual.astype(jnp.float32) + mixer_sum, mix_gain)
    flat_routes = routes.reshape(N_SP, TOK * TOPK).astype(jnp.int32)
    one_hot = (flat_routes[:, :, None] == jnp.arange(EXPERTS, dtype=jnp.int32)[None, None, :]).astype(jnp.int32)
    rank_table = jnp.cumsum(one_hot, axis=1) - one_hot
    slot_index = lax.optimization_barrier(jnp.sum(rank_table * one_hot, axis=2)).astype(jnp.int32)
    blocks = jnp.broadcast_to(jnp.arange(N_SP, dtype=jnp.int32)[:, None], flat_routes.shape)
    source = blocks * TOK + jnp.arange(TOK * TOPK, dtype=jnp.int32)[None, :] // TOPK
    buffer = jnp.zeros((EXPERTS, N_SP, CAP, D), jnp.bfloat16).at[flat_routes, blocks, slot_index].set(normed[source])

    def one_expert(operands):
        rows_in, weight_gate, weight_up, weight_down = operands
        rows_in = rows_in.reshape(N_SP * CAP, D)
        gate_pre = jnp.dot(rows_in, weight_gate, preferred_element_type=jnp.float32)
        up_pre = jnp.dot(rows_in, weight_up, preferred_element_type=jnp.float32)
        hidden = clamped_unit(gate_pre, up_pre)
        expert_out = jnp.dot(hidden, weight_down, preferred_element_type=jnp.float32).astype(jnp.bfloat16)
        return expert_out.reshape(N_SP, CAP, D)
    results = lax.map(one_expert, (buffer, expert_gate, expert_up, expert_down))
    picked = results[flat_routes, blocks, slot_index].astype(jnp.float32).reshape(TOKENS, TOPK, D)
    ffn_out = lax.optimization_barrier(jnp.sum(picked * route_weight[:, :, None], axis=1))
    return layer_norm(ALPHA * normed.astype(jnp.float32) + ffn_out, ffn_gain)
```

```python
import jax
import jax.numpy as jnp
from jax import lax
from jax.experimental import pallas as pl
from jax.experimental.pallas import tpu as pltpu
from jax.sharding import Mesh
from jax.sharding import PartitionSpec as P

D = 2048
CAP = 32
ALPHA = 8.0**0.25
EPSILON = 1e-05
LIMIT = 7.0
SLOPE = 1.702
MESH_ID = pl.DeviceIdType.MESH
BF = jnp.bfloat16
F32 = jnp.float32

NZ, NC, NY, NX = 16, 2, 4, 4
NSP = NZ * NC
ROWS = NSP * CAP
GROUPS = 4
GR = ROWS // GROUPS
HALF = GR // 2
QUARTER = HALF // 2
KPG = GR // CAP


def z_shift(k):
    step, side = k // 2, k % 2
    if step == 0:
        return 0, side
    return ((step + 1) // 2 if step % 2 else NZ - step // 2), side


SCHEDULE = [
    ("a0", 0), ("a0", 1), ("a1", 0), ("a1", 1), ("a2", 0), ("a0", 2), ("a2", 1), ("a1", 2),
    ("a3", 0), ("a0", 3), ("a1", 3), ("c", 0), ("a3", 1), ("a2", 2), ("r1", 0), ("c", 1),
    ("a3", 2), ("a2", 3), ("r2", 0), ("r1", 1), ("c", 2), ("a3", 3), ("r3", 0), ("r2", 1),
    ("r1", 2), ("c", 3), ("r4", 0), ("r3", 1), ("r2", 2), ("r1", 3), ("r4", 1), ("r3", 2),
    ("r2", 3), ("r4", 2), ("r3", 3), ("r4", 3),
]


def column_of(row_ref, size):
    eye = lax.broadcasted_iota(jnp.int32, (size, size), 0) == lax.broadcasted_iota(
        jnp.int32, (size, size), 1
    )
    row = jnp.broadcast_to(row_ref, (size, size))
    return jnp.sum(jnp.where(eye, row, 0.0), axis=1, keepdims=True)


def nt_dot(a, b, dims):
    return lax.dot_general(a, b, (dims, ((), ())), preferred_element_type=F32)


def kernel(
    og, ig, ci, taps, ow, res, doc, mg, fg, routes, rw, wg, wu, wdi,
    out,
    halo, co, wc, wd, st, sp0, sp1, sb, x4, p4, ra1, ra2, rb1, rb2, q, r21, r22, ob, ret, fst,
    nrm, hs, ows, cos, sts, st2s, wds, zs, rets, ags, rss,
):
    z, c = lax.axis_index("z"), lax.axis_index("c")
    y, x = lax.axis_index("y"), lax.axis_index("x")
    own = y * NX + x
    pending = []

    def send(src, dst, sems, index, target):
        copy = pltpu.make_async_remote_copy(
            src_ref=src,
            dst_ref=dst,
            send_sem=sems.at[(0,) + index],
            recv_sem=sems.at[(1,) + index],
            device_id=target,
            device_id_type=MESH_ID,
        )
        copy.start()
        pending.append(copy)

    def landed(dst, sems, index):
        pltpu.make_async_remote_copy(
            src_ref=dst,
            dst_ref=dst,
            send_sem=sems.at[(0,) + index],
            recv_sem=sems.at[(1,) + index],
            device_id=(z, c, y, lax.rem(x + 1, NX)),
            device_id_type=MESH_ID,
        ).wait_recv()

    def in_plane(p):
        return lax.rem(y + p // NX, NY), lax.rem(x + p % NX, NX)

    def from_plane(p):
        return lax.rem(y + NY - p // NX, NY), lax.rem(x + NX - p % NX, NX)

    def along_z(k):
        dz, dc = z_shift(k)
        return (lax.rem(z + dz, NZ), lax.rem(c + dc, NC), y, x)

    def back_z(k):
        dz, dc = z_shift(k)
        return (lax.rem(z + NZ - dz, NZ), lax.rem(c + NC - dc, NC), y, x)

    barrier = pltpu.get_barrier_semaphore()
    for p in range(1, NY * NX):
        py, px = in_plane(p)
        pl.semaphore_signal(barrier, inc=1, device_id=(z, c, py, px), device_id_type=MESH_ID)
    for k in range(1, NSP):
        pl.semaphore_signal(barrier, inc=1, device_id=along_z(k), device_id_type=MESH_ID)

    product = ig[...].astype(F32) * ci[...].astype(F32)
    marks = doc[...].astype(F32)
    halo[0, 0:32, :] = product[:, 128:256]
    halo[0, 32:40, :] = jnp.broadcast_to(marks[:, 128:256], (8, 128))
    tap = [column_of(taps[i : i + 1, :], 32) for i in range(3)]
    ids = lax.broadcasted_iota(jnp.int32, (NSP, 256), 0)
    hits = [(routes[i : i + 1, :] == ids).astype(F32) for i in range(2)]
    before = (
        lax.broadcasted_iota(jnp.int32, (256, 256), 0)
        < lax.broadcasted_iota(jnp.int32, (256, 256), 1)
    ).astype(F32)
    counts = jnp.dot(
        (hits[0] + hits[1]).astype(BF), before.astype(BF), preferred_element_type=F32
    )
    slots = lax.broadcasted_iota(jnp.int32, (ROWS, 256), 0)
    for i, chosen in ((0, sp0), (1, sp1)):
        rank = jnp.sum(hits[i] * counts, axis=0, keepdims=True).astype(jnp.int32)
        expert = routes[i : i + 1, :]
        ez = jnp.right_shift(expert, 1)
        ec = expert - 2 * ez
        dz = ez - z
        dz = jnp.where(dz < 0, dz + NZ, dz)
        dc = jnp.where(ec == c, 0, 1)
        step = jnp.where(dz == 0, 0, jnp.where(dz <= NZ // 2, 2 * dz - 1, 2 * (NZ - dz)))
        slot = (step * 2 + dc) * CAP + rank
        chosen[...] = jnp.where(slots == slot, 1.0, 0.0).astype(BF)

    pl.semaphore_wait(barrier, NY * NX - 1 + NSP - 1)

    send(halo.at[0], halo.at[1], hs, (0,), (lax.rem(z + c, NZ), 1 - c, y, x))
    for p in range(1, NY * NX):
        py, px = in_plane(p)
        there = py * NX + px
        send(
            ow.at[:, pl.ds(pl.multiple_of(there * 128, 128), 128)],
            wc.at[pl.ds(pl.multiple_of(own * 32, 32), 32), :],
            ows, (p,), (z, c, py, px),
        )
    wc[pl.ds(pl.multiple_of(own * 32, 32), 32), :] = ow[
        :, pl.ds(pl.multiple_of(own * 128, 128), 128)
    ]
    landed(halo.at[1], hs, (0,))
    first = jnp.where((z == 0) & (c == 0), 0.0, 1.0)
    lanes = lax.broadcasted_iota(jnp.int32, (32, 256), 1)
    lane_row = lax.broadcasted_iota(jnp.int32, (1, 256), 1)
    prior = halo[1, 0:32, :]
    prior_mark = halo[1, 32:33, :]
    prior_full = jnp.concatenate([prior, prior], axis=1)
    mark_full = jnp.concatenate([prior_mark, prior_mark], axis=1)
    mixed = tap[2] * product
    for shift in (1, 2):
        back = jnp.where(
            lanes < shift, pltpu.roll(prior_full, shift, 1), pltpu.roll(product, shift, 1)
        )
        back_mark = jnp.where(
            lane_row < shift, pltpu.roll(mark_full, shift, 1), pltpu.roll(marks, shift, 1)
        )
        same = jnp.where(back_mark == marks, 1.0, 0.0)
        same = jnp.where(lane_row < shift, same * first, same)
        mixed = mixed + (same * tap[2 - shift]) * back
    my_rows = pl.ds(pl.multiple_of(own * 32, 32), 32)
    co[my_rows, :] = (og[...].astype(F32) * mixed).astype(BF)
    for p in range(1, NY * NX):
        py, px = in_plane(p)
        send(co.at[my_rows, :], co.at[my_rows, :], cos, (p,), (z, c, py, px))
    stream_t = ALPHA * res[...].astype(F32).T

    def send_down(group):
        for p in group:
            py, px = in_plane(p)
            there = py * NX + px
            send(
                wdi.at[pl.ds(pl.multiple_of(there * 256, 256), 256), :],
                wd.at[:, pl.ds(pl.multiple_of(own * 128, 128), 128)],
                wds, (p,), (z, c, py, px),
            )

    wd[:, pl.ds(pl.multiple_of(own * 128, 128), 128)] = wdi[
        pl.ds(pl.multiple_of(own * 256, 256), 256), :
    ]
    for p in range(1, NY * NX):
        fy, fx = from_plane(p)
        rows = pl.ds(pl.multiple_of((fy * NX + fx) * 32, 32), 32)
        landed(wc.at[rows, :], ows, (p,))
    for p in range(1, NY * NX):
        fy, fx = from_plane(p)
        rows = pl.ds(pl.multiple_of((fy * NX + fx) * 32, 32), 32)
        landed(co.at[rows, :], cos, (p,))
    stream_t = stream_t + nt_dot(wc[...], co[...], ((0,), (0,)))

    def norm(stream, which, sems, gain_col):
        s1 = jnp.sum(stream, axis=0, keepdims=True)
        s2 = jnp.sum(stream * stream, axis=0, keepdims=True)
        sub = lax.broadcasted_iota(jnp.int32, (8, 256), 0)
        st[which, own] = jnp.where(sub == 0, s1, s2)
        for p in range(1, NY * NX):
            py, px = in_plane(p)
            send(st.at[which, own], st.at[which, own], sems, (p,), (z, c, py, px))
        if which == 0:
            send_down(range(1, NY * NX))
        for p in range(1, NY * NX):
            fy, fx = from_plane(p)
            landed(st.at[which, fy * NX + fx], sems, (p,))
        total = st[which, 0]
        for j in range(1, NY * NX):
            total = total + st[which, j]
        mean = total[0:1, :] / D
        spread = total[1:2, :] / D - mean * mean
        return (stream - mean) * lax.rsqrt(spread + EPSILON) * gain_col

    normed_t = norm(stream_t, 0, sts, column_of(mg[...], 128)).astype(BF)
    nrm[...] = normed_t

    for g in range(GROUPS):
        rows = pl.ds(g * GR, GR)
        chosen = sp0[rows, :] + sp1[rows, :]
        sb[rows, :] = nt_dot(chosen, normed_t, ((1,), (1,))).astype(BF)
        for k in range(g * KPG, (g + 1) * KPG):
            cut = pl.ds(k * CAP, CAP)
            if k == 0:
                x4[y, x, cut, :] = sb[cut, :]
            else:
                send(sb.at[cut, :], x4.at[y, x, cut, :], zs, (k,), along_z(k))
    for p in range(1, NY * NX):
        fy, fx = from_plane(p)
        cols = pl.ds(pl.multiple_of((fy * NX + fx) * 128, 128), 128)
        landed(wd.at[:, cols], wds, (p,))

    def ring(axis, step):
        if axis == "x":
            return (z, c, y, lax.rem(x + step + NX, NX))
        return (z, c, lax.rem(y + step + NY, NY), x)

    def spot(axis, step):
        return lax.rem((x if axis == "x" else y) + step + 4, 4)

    def span(g, half, part):
        start = g * GR + half * HALF
        if part == "lo":
            return pl.ds(start, QUARTER)
        if part == "hi":
            return pl.ds(start + QUARTER, QUARTER)
        return pl.ds(start, HALF)

    def slab(buf, g, half, phase, step, part=None):
        rows = span(g, half, part)
        if half == 0:
            if phase == 0:
                return buf.at[y, spot("x", step), rows, :]
            return buf.at[spot("y", step), :, rows, :]
        if phase == 0:
            return buf.at[spot("y", step), x, rows, :]
        return buf.at[:, spot("x", step), rows, :]

    def axis_of(half, phase):
        return "xy"[(half + phase) % 2]

    def ag_send(g, phase):
        for half in range(2):
            axis = axis_of(half, phase)
            base = half * 8 + phase * 4
            mine = slab(x4, g, half, phase, 0)
            send(mine, mine, ags, (g, base), ring(axis, 1))
            send(mine, mine, ags, (g, base + 1), ring(axis, -1))

    def ag_relay(g, phase):
        for half in range(2):
            axis = axis_of(half, phase)
            base = half * 8 + phase * 4
            landed(slab(x4, g, half, phase, -1), ags, (g, base))
            low = slab(x4, g, half, phase, -1, "lo")
            send(low, low, ags, (g, base + 2), ring(axis, 1))
            landed(slab(x4, g, half, phase, 1), ags, (g, base + 1))
            high = slab(x4, g, half, phase, 1, "hi")
            send(high, high, ags, (g, base + 3), ring(axis, -1))

    def ag_end(g, phase):
        for half in range(2):
            base = half * 8 + phase * 4
            landed(slab(x4, g, half, phase, 2, "lo"), ags, (g, base + 2))
            landed(slab(x4, g, half, phase, 2, "hi"), ags, (g, base + 3))

    def compute(g):
        rows = pl.ds(g * GR, GR)
        inputs = jnp.concatenate(
            [x4[b, a, rows, :] for b in range(NY) for a in range(NX)], axis=1
        )
        gate = jnp.minimum(jnp.dot(inputs, wg[...], preferred_element_type=F32), LIMIT)
        up = jnp.clip(jnp.dot(inputs, wu[...], preferred_element_type=F32), -LIMIT, LIMIT)
        hidden = ((up + 1.0) * gate * jax.nn.sigmoid(SLOPE * gate)).astype(BF)
        for b in range(NY):
            part = jnp.dot(
                hidden, wd[:, b * 512 : (b + 1) * 512], preferred_element_type=F32
            ).astype(BF)
            for a in range(NX):
                p4[b, a, rows, :] = part[:, a * 128 : (a + 1) * 128]

    first_in = (ra1, rb1)
    second_in = (ra2, rb2)

    def rs_first(g, phase):
        for half in range(2):
            axis = axis_of(half, 1 - phase)
            base = half * 8 + phase * 4
            for way, part in ((0, "lo"), (1, "hi")):
                if phase == 0:
                    src = slab(p4, g, half, 1, 2, part)
                    dst = first_in[half].at[g, way]
                else:
                    cut = pl.ds(way * QUARTER, QUARTER)
                    src = q.at[g, half, spot(axis, 2), cut, :]
                    dst = r21.at[g, half, way]
                send(src, dst, rss, (g, base + way), ring(axis, 1 - 2 * way))

    def rs_second(g, phase):
        for half in range(2):
            axis = axis_of(half, 1 - phase)
            base = half * 8 + phase * 4
            for way, part in ((0, "lo"), (1, "hi")):
                step = 1 - 2 * way
                if phase == 0:
                    came = first_in[half].at[g, way]
                    edge = slab(p4, g, half, 1, step, part)
                    whole = slab(p4, g, half, 1, step)
                    dst = second_in[half].at[g, way]
                else:
                    came = r21.at[g, half, way]
                    cut = pl.ds(way * QUARTER, QUARTER)
                    edge = q.at[g, half, spot(axis, step), cut, :]
                    whole = q.at[g, half, spot(axis, step)]
                    dst = r22.at[g, half, way]
                landed(came, rss, (g, base + way))
                edge[...] = (edge[...].astype(F32) + came[...].astype(F32)).astype(BF)
                send(whole, dst, rss, (g, base + 2 + way), ring(axis, step))

    def rs_end(g, phase):
        for half in range(2):
            base = half * 8 + phase * 4
            axis = axis_of(half, 1 - phase)
            for way in range(2):
                dst = (second_in[half] if phase == 0 else r22.at[:, half]).at[g, way]
                landed(dst, rss, (g, base + 2 + way))
            if phase == 0:
                mine = slab(p4, g, half, 1, 0)
                fwd, bwd = second_in[half].at[g, 0], second_in[half].at[g, 1]
                q[g, half] = (
                    mine[...].astype(F32) + fwd[...].astype(F32) + bwd[...].astype(F32)
                ).astype(BF)
            else:
                rows = span(g, half, None)
                ob[rows, :] = (
                    q[g, half, spot(axis, 0)].astype(F32)
                    + r22[g, half, 0].astype(F32)
                    + r22[g, half, 1].astype(F32)
                ).astype(BF)

    for stage, g in SCHEDULE:
        if stage == "a0":
            for k in range(g * KPG, (g + 1) * KPG):
                if k > 0:
                    landed(x4.at[y, x, pl.ds(k * CAP, CAP), :], zs, (k,))
            ag_send(g, 0)
        elif stage == "a1":
            ag_relay(g, 0)
        elif stage == "a2":
            ag_end(g, 0)
            ag_send(g, 1)
        elif stage == "a3":
            ag_relay(g, 1)
        elif stage == "c":
            ag_end(g, 1)
            compute(g)
            rs_first(g, 0)
        elif stage == "r1":
            rs_second(g, 0)
        elif stage == "r2":
            rs_end(g, 0)
            rs_first(g, 1)
        elif stage == "r3":
            rs_second(g, 1)
        else:
            rs_end(g, 1)
            for k in range(g * KPG, (g + 1) * KPG):
                cut = pl.ds(k * CAP, CAP)
                if k == 0:
                    ret[cut, :] = ob[cut, :]
                else:
                    send(ob.at[cut, :], ret.at[cut, :], rets, (k,), back_z(k))

    for k in range(1, NSP):
        landed(ret.at[pl.ds(k * CAP, CAP), :], rets, (k,))
    results = ret[...]
    ffn = rw[0:1, :] * nt_dot(results, sp0[...], ((0,), (0,)))
    ffn = ffn + rw[1:2, :] * nt_dot(results, sp1[...], ((0,), (0,)))
    second = ALPHA * nrm[...].astype(F32) + ffn
    out[...] = norm(second, 1, st2s, column_of(fg[...], 128)).T.astype(BF)
    for copy in pending:
        copy.wait_send()


def per_device(
    out_gate, in_gate, conv_input, conv_taps, out_weight, residual, document, mix_gain,
    ffn_gain, routes, route_weight, expert_gate, expert_up, expert_down,
):
    vmem = pl.BlockSpec(memory_space=pltpu.VMEM)
    dma = pltpu.SemaphoreType.DMA
    scratch = [
        pltpu.VMEM((2, 40, 128), F32),
        pltpu.VMEM((512, 256), BF),
        pltpu.VMEM((512, 128), BF),
        pltpu.VMEM((256, D), BF),
        pltpu.VMEM((2, 16, 8, 256), F32),
        pltpu.VMEM((ROWS, 256), BF),
        pltpu.VMEM((ROWS, 256), BF),
        pltpu.VMEM((ROWS, 128), BF),
        pltpu.VMEM((NY, NX, ROWS, 128), BF),
        pltpu.VMEM((NY, NX, ROWS, 128), BF),
        pltpu.VMEM((GROUPS, 2, 4, QUARTER, 128), BF),
        pltpu.VMEM((GROUPS, 2, 4, HALF, 128), BF),
        pltpu.VMEM((GROUPS, 2, 4, QUARTER, 128), BF),
        pltpu.VMEM((GROUPS, 2, 4, HALF, 128), BF),
        pltpu.VMEM((GROUPS, 2, 4, HALF, 128), BF),
        pltpu.VMEM((GROUPS, 2, 2, QUARTER, 128), BF),
        pltpu.VMEM((GROUPS, 2, 2, HALF, 128), BF),
        pltpu.VMEM((ROWS, 128), BF),
        pltpu.VMEM((ROWS, 128), BF),
        pltpu.VMEM((8, 128), F32),
        pltpu.VMEM((128, 256), BF),
        dma((2, 1)),
        dma((2, 16)),
        dma((2, 16)),
        dma((2, 16)),
        dma((2, 16)),
        dma((2, 16)),
        dma((2, NSP)),
        dma((2, NSP)),
        dma((2, GROUPS, 16)),
        dma((2, GROUPS, 16)),
    ]
    return pl.pallas_call(
        kernel,
        out_shape=jax.ShapeDtypeStruct((256, 128), BF),
        in_specs=[vmem] * 14,
        out_specs=vmem,
        scratch_shapes=scratch,
        compiler_params=pltpu.CompilerParams(
            collective_id=0, has_side_effects=True, vmem_limit_bytes=60 * 1024 * 1024
        ),
    )(
        out_gate.T, in_gate.T, conv_input.T, conv_taps, out_weight, residual,
        document[None, :], mix_gain[None, :], ffn_gain[None, :], routes.T, route_weight.T,
        expert_gate[0], expert_up[0], expert_down[0],
    )


def solution(mesh):
    torus = Mesh(mesh.devices.reshape(NZ, NC, NY, NX), ("z", "c", "y", "x"))
    sp, tp = ("z", "c"), ("y", "x")
    in_specs = (
        P(sp, tp), P(sp, tp), P(sp, tp), P(None, tp), P(tp, None), P(sp, tp), P(sp), P(tp),
        P(tp), P(sp, None), P(sp, None), P(sp, None, tp), P(sp, None, tp), P(sp, None, tp),
    )
    return jax.shard_map(
        per_device, mesh=torus, in_specs=in_specs, out_specs=P(sp, tp), check_vma=False
    )
```

```python
import jax
import jax.numpy as jnp
from jax import lax
from jax.experimental import pallas as pl
from jax.experimental.pallas import tpu as pltpu
from jax.sharding import Mesh
from jax.sharding import PartitionSpec as P

D = 2048
CAP = 32
ALPHA = 8.0**0.25
EPSILON = 1e-05
LIMIT = 7.0
SLOPE = 1.702
MESH_ID = pl.DeviceIdType.MESH
BF = jnp.bfloat16
F32 = jnp.float32

NZ, NC, NY, NX = 16, 2, 4, 4
NSP = NZ * NC
ROWS = NSP * CAP
GROUPS = 4
GR = ROWS // GROUPS
HALF = GR // 2
QUARTER = HALF // 2
KPG = GR // CAP


def z_shift(k):
    step, side = k // 2, k % 2
    step = PERM[step // 4] * 4 + step % 4
    if step == 0:
        return 0, side
    return ((step + 1) // 2 if step % 2 else NZ - step // 2), side


PERM = (0, 2, 3, 1)
SCHEDULE = [
    ("a0", 0), ("a1", 0), ("a0", 1), ("a2", 0), ("a0", 2), ("a1", 1), ("a0", 3), ("a3", 0),
    ("a1", 3), ("a1", 2), ("a2", 1), ("a2", 2), ("a2", 3), ("c", 0), ("a3", 1), ("a3", 2),
    ("a3", 3), ("h1", 0), ("c", 1), ("c", 2), ("c", 3), ("d", 0), ("h1", 1), ("h1", 2),
    ("h1", 3), ("e1", 0), ("d", 1), ("d", 2), ("d", 3), ("e1", 1), ("e2", 0), ("e1", 2),
    ("e1", 3), ("e2", 1), ("e2", 2), ("e2", 3),
]


def column_of(row_ref, size):
    eye = lax.broadcasted_iota(jnp.int32, (size, size), 0) == lax.broadcasted_iota(
        jnp.int32, (size, size), 1
    )
    row = jnp.broadcast_to(row_ref, (size, size))
    return jnp.sum(jnp.where(eye, row, 0.0), axis=1, keepdims=True)


def nt_dot(a, b, dims):
    return lax.dot_general(a, b, (dims, ((), ())), preferred_element_type=F32)


def kernel(
    og, ig, ci, taps, ow, res, doc, mg, fg, routes, rw, wgh, wuh, wdh,
    out,
    wg, wu, wdi, halo, co, wc, wda, wdb, wra, wrb, st, sp0, sp1, sb, x4, h4, p4, r1, r2, ob, ret,
    nrm, ls, hs, ows, cos, sts, st2s, wds, zs, rets, ags, hds, rss,
):
    z, c = lax.axis_index("z"), lax.axis_index("c")
    y, x = lax.axis_index("y"), lax.axis_index("x")
    own = y * NX + x
    pending = []

    def send(src, dst, sems, index, target):
        copy = pltpu.make_async_remote_copy(
            src_ref=src,
            dst_ref=dst,
            send_sem=sems.at[(0,) + index],
            recv_sem=sems.at[(1,) + index],
            device_id=target,
            device_id_type=MESH_ID,
        )
        copy.start()
        pending.append(copy)

    def landed(dst, sems, index):
        pltpu.make_async_remote_copy(
            src_ref=dst,
            dst_ref=dst,
            send_sem=sems.at[(0,) + index],
            recv_sem=sems.at[(1,) + index],
            device_id=(z, c, y, lax.rem(x + 1, NX)),
            device_id_type=MESH_ID,
        ).wait_recv()

    def in_plane(p):
        return lax.rem(y + p // NX, NY), lax.rem(x + p % NX, NX)

    def from_plane(p):
        return lax.rem(y + NY - p // NX, NY), lax.rem(x + NX - p % NX, NX)

    def along_z(k):
        dz, dc = z_shift(k)
        return (lax.rem(z + dz, NZ), lax.rem(c + dc, NC), y, x)

    def back_z(k):
        dz, dc = z_shift(k)
        return (lax.rem(z + NZ - dz, NZ), lax.rem(c + NC - dc, NC), y, x)

    barrier = pltpu.get_barrier_semaphore()
    loads = [
        pltpu.make_async_copy(wdh, wdi, ls.at[0]),
        pltpu.make_async_copy(wgh, wg, ls.at[1]),
        pltpu.make_async_copy(wuh, wu, ls.at[2]),
    ]
    for load in loads:
        load.start()
    with jax.named_scope("signals"):
        for p in range(1, NY * NX):
            py, px = in_plane(p)
            pl.semaphore_signal(barrier, inc=1, device_id=(z, c, py, px), device_id_type=MESH_ID)
        for k in range(1, NSP):
            pl.semaphore_signal(barrier, inc=1, device_id=along_z(k), device_id_type=MESH_ID)

    with jax.named_scope("local"):
        product = ig[...].astype(F32) * ci[...].astype(F32)
        marks = doc[...].astype(F32)
        halo[0, 0:32, :] = product[:, 128:256]
        halo[0, 32:40, :] = jnp.broadcast_to(marks[:, 128:256], (8, 128))
        tap = [column_of(taps[i : i + 1, :], 32) for i in range(3)]
        ids = lax.broadcasted_iota(jnp.int32, (NSP, 256), 0)
        hits = [(routes[i : i + 1, :] == ids).astype(F32) for i in range(2)]
        before = (
            lax.broadcasted_iota(jnp.int32, (256, 256), 0)
            < lax.broadcasted_iota(jnp.int32, (256, 256), 1)
        ).astype(F32)
        counts = jnp.dot(
            (hits[0] + hits[1]).astype(BF), before.astype(BF), preferred_element_type=F32
        )
        slots = lax.broadcasted_iota(jnp.int32, (ROWS, 256), 0)
        for i, chosen in ((0, sp0), (1, sp1)):
            rank = jnp.sum(hits[i] * counts, axis=0, keepdims=True).astype(jnp.int32)
            expert = routes[i : i + 1, :]
            ez = jnp.right_shift(expert, 1)
            ec = expert - 2 * ez
            dz = ez - z
            dz = jnp.where(dz < 0, dz + NZ, dz)
            dc = jnp.where(ec == c, 0, 1)
            step = jnp.where(dz == 0, 0, jnp.where(dz <= NZ // 2, 2 * dz - 1, 2 * (NZ - dz)))
            block = jnp.right_shift(step, 2)
            place = jnp.zeros_like(block)
            for here, there in enumerate(PERM):
                place = jnp.where(block == there, here, place)
            step = place * 4 + (step - block * 4)
            slot = (step * 2 + dc) * CAP + rank
            chosen[...] = jnp.where(slots == slot, 1.0, 0.0).astype(BF)

    with jax.named_scope("entry"):
        pl.semaphore_wait(barrier, NY * NX - 1 + NSP - 1)

    with jax.named_scope("halo_send"):
        send(halo.at[0], halo.at[1], hs, (0,), (lax.rem(z + c, NZ), 1 - c, y, x))
        for p in range(1, NY * NX):
            py, px = in_plane(p)
            there = py * NX + px
            send(
                ow.at[:, pl.ds(pl.multiple_of(there * 128, 128), 128)],
                wc.at[pl.ds(pl.multiple_of(own * 32, 32), 32), :],
                ows, (p,), (z, c, py, px),
            )
        wc[pl.ds(pl.multiple_of(own * 32, 32), 32), :] = ow[
            :, pl.ds(pl.multiple_of(own * 128, 128), 128)
        ]
    with jax.named_scope("halo_wait"):
        landed(halo.at[1], hs, (0,))
    with jax.named_scope("conv"):
        first = jnp.where((z == 0) & (c == 0), 0.0, 1.0)
        lanes = lax.broadcasted_iota(jnp.int32, (32, 256), 1)
        lane_row = lax.broadcasted_iota(jnp.int32, (1, 256), 1)
        prior = halo[1, 0:32, :]
        prior_mark = halo[1, 32:33, :]
        prior_full = jnp.concatenate([prior, prior], axis=1)
        mark_full = jnp.concatenate([prior_mark, prior_mark], axis=1)
        mixed = tap[2] * product
        for shift in (1, 2):
            back = jnp.where(
                lanes < shift, pltpu.roll(prior_full, shift, 1), pltpu.roll(product, shift, 1)
            )
            back_mark = jnp.where(
                lane_row < shift, pltpu.roll(mark_full, shift, 1), pltpu.roll(marks, shift, 1)
            )
            same = jnp.where(back_mark == marks, 1.0, 0.0)
            same = jnp.where(lane_row < shift, same * first, same)
            mixed = mixed + (same * tap[2 - shift]) * back
        my_rows = pl.ds(pl.multiple_of(own * 32, 32), 32)
        co[my_rows, :] = (og[...].astype(F32) * mixed).astype(BF)
        for p in range(1, NY * NX):
            py, px = in_plane(p)
            send(co.at[my_rows, :], co.at[my_rows, :], cos, (p,), (z, c, py, px))
    with jax.named_scope("residual"):
        stream_t = ALPHA * res[...].astype(F32).T

    def ring(axis, step):
        if axis == "x":
            return (z, c, y, lax.rem(x + step + NX, NX))
        return (z, c, lax.rem(y + step + NY, NY), x)

    def spot(axis, step):
        return lax.rem((x if axis == "x" else y) + step + 4, 4)

    def down_rows(half, step, part=None):
        lead = spot("yx"[half], step)
        if half == 0:
            return wdi.at[lead] if part is None else wdi.at[lead, pl.ds(2 * part, 2)]
        return wdi.at[:, lead] if part is None else wdi.at[pl.ds(2 * part, 2), lead]

    def down_cols(half, step, part=None):
        cols = pl.ds(pl.multiple_of(spot("yx"[half], step) * 128, 128), 128)
        buf = (wda, wdb)[half]
        return buf.at[:, :, cols] if part is None else buf.at[pl.ds(2 * part, 2), :, cols]

    def down_first():
        loads[0].wait()
        for half in range(2):
            for way in range(2):
                step = 1 - 2 * way
                send(
                    down_rows(half, step), down_cols(half, 0), wds, (half * 6 + way,),
                    ring("yx"[half], step),
                )

    def down_relayed():
        for half in range(2):
            for way in range(2):
                send(
                    down_rows(half, 2, way), (wra, wrb)[half].at[way], wds,
                    (half * 6 + 2 + way,), ring("yx"[half], 1 - 2 * way),
                )

    def down_relay():
        for half in range(2):
            for way in range(2):
                step = 1 - 2 * way
                came = (wra, wrb)[half].at[way]
                landed(came, wds, (half * 6 + 2 + way,))
                send(
                    came, down_cols(half, -step, way), wds, (half * 6 + 4 + way,),
                    ring("yx"[half], step),
                )

    def down_end():
        for half in range(2):
            for way in range(2):
                step = 1 - 2 * way
                landed(down_cols(half, -step), wds, (half * 6 + way,))
                landed(down_cols(half, 2, way), wds, (half * 6 + 4 + way,))

    with jax.named_scope("down_first"):
        down_first()
        own_y = pl.ds(pl.multiple_of(y * 128, 128), 128)
        own_x = pl.ds(pl.multiple_of(x * 128, 128), 128)
        wda[:, :, own_y] = wdi[y]
        wdb[:, :, own_x] = wdi[:, x]
    with jax.named_scope("mix_wait"):
        for p in range(1, NY * NX):
            fy, fx = from_plane(p)
            rows = pl.ds(pl.multiple_of((fy * NX + fx) * 32, 32), 32)
            landed(wc.at[rows, :], ows, (p,))
        for p in range(1, NY * NX):
            fy, fx = from_plane(p)
            rows = pl.ds(pl.multiple_of((fy * NX + fx) * 32, 32), 32)
            landed(co.at[rows, :], cos, (p,))
    with jax.named_scope("mix_dot"):
        stream_t = stream_t + nt_dot(wc[...], co[...], ((0,), (0,)))

    def norm(stream, which, sems, gain_col):
        s1 = jnp.sum(stream, axis=0, keepdims=True)
        s2 = jnp.sum(stream * stream, axis=0, keepdims=True)
        sub = lax.broadcasted_iota(jnp.int32, (2, 256), 0)
        st[which, own] = jnp.where(sub == 0, s1, s2)
        for p in range(1, NY * NX):
            py, px = in_plane(p)
            send(st.at[which, own], st.at[which, own], sems, (p,), (z, c, py, px))
        if which == 0:
            down_relayed()
        for p in range(1, NY * NX):
            fy, fx = from_plane(p)
            landed(st.at[which, fy * NX + fx], sems, (p,))
        total = st[which, 0]
        for j in range(1, NY * NX):
            total = total + st[which, j]
        mean = total[0:1, :] / D
        spread = total[1:2, :] / D - mean * mean
        return (stream - mean) * lax.rsqrt(spread + EPSILON) * gain_col

    with jax.named_scope("norm_a"):
        normed_t = norm(stream_t, 0, sts, column_of(mg[...], 128)).astype(BF)
    nrm[...] = normed_t

    with jax.named_scope("dispatch"):
        for g in range(GROUPS):
            rows = pl.ds(g * GR, GR)
            chosen = sp0[rows, :] + sp1[rows, :]
            sb[rows, :] = nt_dot(chosen, normed_t, ((1,), (1,))).astype(BF)
            for k in range(g * KPG, (g + 1) * KPG):
                cut = pl.ds(k * CAP, CAP)
                if k == 0:
                    x4[y, x, cut, :] = sb[cut, :]
                else:
                    send(sb.at[cut, :], x4.at[y, x, cut, :], zs, (k,), along_z(k))
    with jax.named_scope("down_relay"):
        down_relay()

    def span(g, half, part):
        start = g * GR + half * HALF
        if part == "lo":
            return pl.ds(start, QUARTER)
        if part == "hi":
            return pl.ds(start + QUARTER, QUARTER)
        return pl.ds(start, HALF)

    def slab(buf, g, half, phase, step, part=None):
        rows = span(g, half, part)
        if half == 0:
            if phase == 0:
                return buf.at[y, spot("x", step), rows, :]
            return buf.at[spot("y", step), :, rows, :]
        if phase == 0:
            return buf.at[spot("y", step), x, rows, :]
        return buf.at[:, spot("x", step), rows, :]

    def axis_of(half, phase):
        return "xy"[(half + phase) % 2]

    def ag_send(g, phase):
        for half in range(2):
            axis = axis_of(half, phase)
            base = half * 8 + phase * 4
            mine = slab(x4, g, half, phase, 0)
            send(mine, mine, ags, (g, base), ring(axis, 1))
            send(mine, mine, ags, (g, base + 1), ring(axis, -1))

    def ag_relay(g, phase):
        for half in range(2):
            axis = axis_of(half, phase)
            base = half * 8 + phase * 4
            landed(slab(x4, g, half, phase, -1), ags, (g, base))
            low = slab(x4, g, half, phase, -1, "lo")
            send(low, low, ags, (g, base + 2), ring(axis, 1))
            landed(slab(x4, g, half, phase, 1), ags, (g, base + 1))
            high = slab(x4, g, half, phase, 1, "hi")
            send(high, high, ags, (g, base + 3), ring(axis, -1))

    def ag_end(g, phase):
        for half in range(2):
            base = half * 8 + phase * 4
            landed(slab(x4, g, half, phase, 2, "lo"), ags, (g, base + 2))
            landed(slab(x4, g, half, phase, 2, "hi"), ags, (g, base + 3))

    def expert_in(g):
        rows = pl.ds(g * GR, GR)
        inputs = jnp.concatenate(
            [x4[b, a, rows, :] for b in range(NY) for a in range(NX)], axis=1
        )
        gate = jnp.minimum(jnp.dot(inputs, wg[...], preferred_element_type=F32), LIMIT)
        up = jnp.clip(jnp.dot(inputs, wu[...], preferred_element_type=F32), -LIMIT, LIMIT)
        hidden = ((up + 1.0) * gate * jax.nn.sigmoid(SLOPE * gate)).astype(BF)
        for half in range(2):
            h4[spot("xy"[half], 0), span(g, half, None), :] = hidden[
                half * HALF : (half + 1) * HALF, :
            ]

    def hidden_at(g, half, step, part=None):
        return h4.at[spot("xy"[half], step), span(g, half, part), :]

    def hidden_send(g):
        for half in range(2):
            for way in range(2):
                mine = hidden_at(g, half, 0)
                send(mine, mine, hds, (g, half * 4 + way), ring("xy"[half], 1 - 2 * way))

    def hidden_relay(g):
        for half in range(2):
            for way, part in ((0, "lo"), (1, "hi")):
                step = 1 - 2 * way
                landed(hidden_at(g, half, -step), hds, (g, half * 4 + way))
                piece = hidden_at(g, half, -step, part)
                send(piece, piece, hds, (g, half * 4 + 2 + way), ring("xy"[half], step))

    def hidden_end(g):
        for half in range(2):
            for way, part in ((0, "lo"), (1, "hi")):
                landed(hidden_at(g, half, 2, part), hds, (g, half * 4 + 2 + way))

    def expert_out(g):
        for half in range(2):
            rows = span(g, half, None)
            inputs = jnp.concatenate([h4[b, rows, :] for b in range(4)], axis=1)
            weights = (wda, wdb)[half][...].reshape(1024, 512)
            part = jnp.dot(inputs, weights, preferred_element_type=F32).astype(BF)
            for b in range(4):
                p4[b, rows, :] = part[:, b * 128 : (b + 1) * 128]

    def part_at(g, half, step, part=None):
        return p4.at[spot("yx"[half], step), span(g, half, part), :]

    def sum_first(g):
        for half in range(2):
            for way, part in ((0, "lo"), (1, "hi")):
                send(
                    part_at(g, half, 2, part), r1.at[g, half, way], rss,
                    (g, half * 4 + way), ring("yx"[half], 1 - 2 * way),
                )

    def sum_second(g):
        for half in range(2):
            for way, part in ((0, "lo"), (1, "hi")):
                step = 1 - 2 * way
                landed(r1.at[g, half, way], rss, (g, half * 4 + way))
                edge = part_at(g, half, step, part)
                edge[...] = (edge[...].astype(F32) + r1[g, half, way].astype(F32)).astype(BF)
                send(
                    part_at(g, half, step), r2.at[g, half, way], rss,
                    (g, half * 4 + 2 + way), ring("yx"[half], step),
                )

    def sum_end(g):
        for half in range(2):
            for way in range(2):
                landed(r2.at[g, half, way], rss, (g, half * 4 + 2 + way))
            ob[span(g, half, None), :] = (
                part_at(g, half, 0)[...].astype(F32)
                + r2[g, half, 0].astype(F32)
                + r2[g, half, 1].astype(F32)
            ).astype(BF)

    for stage, g in SCHEDULE:
        with jax.named_scope(f"{stage}_{g}"):
            if stage == "a0":
                for k in range(g * KPG, (g + 1) * KPG):
                    if k > 0:
                        landed(x4.at[y, x, pl.ds(k * CAP, CAP), :], zs, (k,))
                ag_send(g, 0)
            elif stage == "a1":
                ag_relay(g, 0)
            elif stage == "a2":
                ag_end(g, 0)
                ag_send(g, 1)
            elif stage == "a3":
                ag_relay(g, 1)
            elif stage == "c":
                ag_end(g, 1)
                if g == 0:
                    loads[1].wait()
                    loads[2].wait()
                expert_in(g)
                hidden_send(g)
            elif stage == "h1":
                hidden_relay(g)
            elif stage == "d":
                hidden_end(g)
                if g == 0:
                    down_end()
                expert_out(g)
                sum_first(g)
            elif stage == "e1":
                sum_second(g)
            else:
                sum_end(g)
                for k in range(g * KPG, (g + 1) * KPG):
                    cut = pl.ds(k * CAP, CAP)
                    if k == 0:
                        ret[cut, :] = ob[cut, :]
                    else:
                        send(ob.at[cut, :], ret.at[cut, :], rets, (k,), back_z(k))

    with jax.named_scope("ret_wait"):
        for k in range(1, NSP):
            landed(ret.at[pl.ds(k * CAP, CAP), :], rets, (k,))
    with jax.named_scope("combine"):
        results = ret[...]
        ffn = rw[0:1, :] * nt_dot(results, sp0[...], ((0,), (0,)))
        ffn = ffn + rw[1:2, :] * nt_dot(results, sp1[...], ((0,), (0,)))
        second = ALPHA * nrm[...].astype(F32) + ffn
    with jax.named_scope("norm_b"):
        out[...] = norm(second, 1, st2s, column_of(fg[...], 128)).T.astype(BF)
    for copy in pending:
        copy.wait_send()


def per_device(
    out_gate, in_gate, conv_input, conv_taps, out_weight, residual, document, mix_gain,
    ffn_gain, routes, route_weight, expert_gate, expert_up, expert_down,
):
    vmem = pl.BlockSpec(memory_space=pltpu.VMEM)
    away = pl.BlockSpec(memory_space=pl.ANY)
    dma = pltpu.SemaphoreType.DMA
    scratch = [
        pltpu.VMEM((D, 256), BF),
        pltpu.VMEM((D, 256), BF),
        pltpu.VMEM((NY, NX, 256, 128), BF),
        pltpu.VMEM((2, 40, 128), F32),
        pltpu.VMEM((512, 256), BF),
        pltpu.VMEM((512, 128), BF),
        pltpu.VMEM((4, 256, 512), BF),
        pltpu.VMEM((4, 256, 512), BF),
        pltpu.VMEM((2, 2, 256, 128), BF),
        pltpu.VMEM((2, 2, 256, 128), BF),
        pltpu.VMEM((2, 16, 2, 256), F32),
        pltpu.VMEM((ROWS, 256), BF),
        pltpu.VMEM((ROWS, 256), BF),
        pltpu.VMEM((ROWS, 128), BF),
        pltpu.VMEM((NY, NX, ROWS, 128), BF),
        pltpu.VMEM((4, ROWS, 256), BF),
        pltpu.VMEM((4, ROWS, 128), BF),
        pltpu.VMEM((GROUPS, 2, 2, QUARTER, 128), BF),
        pltpu.VMEM((GROUPS, 2, 2, HALF, 128), BF),
        pltpu.VMEM((ROWS, 128), BF),
        pltpu.VMEM((ROWS, 128), BF),
        pltpu.VMEM((128, 256), BF),
        dma((3,)),
        dma((2, 1)),
        dma((2, 16)),
        dma((2, 16)),
        dma((2, 16)),
        dma((2, 16)),
        dma((2, 12)),
        dma((2, NSP)),
        dma((2, NSP)),
        dma((2, GROUPS, 16)),
        dma((2, GROUPS, 8)),
        dma((2, GROUPS, 8)),
    ]
    return pl.pallas_call(
        kernel,
        out_shape=jax.ShapeDtypeStruct((256, 128), BF),
        in_specs=[vmem] * 11 + [away] * 3,
        out_specs=vmem,
        scratch_shapes=scratch,
        compiler_params=pltpu.CompilerParams(
            collective_id=0, has_side_effects=True, vmem_limit_bytes=60 * 1024 * 1024
        ),
    )(
        out_gate.T, in_gate.T, conv_input.T, conv_taps, out_weight, residual,
        document[None, :], mix_gain[None, :], ffn_gain[None, :], routes.T, route_weight.T,
        expert_gate[0], expert_up[0], expert_down[0].reshape(NY, NX, 256, 128),
    )


def solution(mesh):
    torus = Mesh(mesh.devices.reshape(NZ, NC, NY, NX), ("z", "c", "y", "x"))
    sp, tp = ("z", "c"), ("y", "x")
    in_specs = (
        P(sp, tp), P(sp, tp), P(sp, tp), P(None, tp), P(tp, None), P(sp, tp), P(sp), P(tp),
        P(tp), P(sp, None), P(sp, None), P(sp, None, tp), P(sp, None, tp), P(sp, None, tp),
    )
    return jax.shard_map(
        per_device, mesh=torus, in_specs=in_specs, out_specs=P(sp, tp), check_vma=False
    )
```

```python
import jax
import jax.numpy as jnp
from jax import lax
from jax.experimental import pallas as pl
from jax.experimental.pallas import tpu as pltpu
from jax.sharding import Mesh
from jax.sharding import PartitionSpec as P

D = 2048
CAP = 32
ALPHA = 8.0**0.25
EPSILON = 1e-05
LIMIT = 7.0
SLOPE = 1.702
MESH_ID = pl.DeviceIdType.MESH
BF = jnp.bfloat16
F32 = jnp.float32

NZ, NC, NY, NX = 16, 2, 4, 4
NSP = NZ * NC
ROWS = NSP * CAP
SIZES = (2, 2, 4, 4, 2, 2)
GROUPS = len(SIZES)
STARTS = tuple(sum(SIZES[:g]) for g in range(GROUPS))
ORDER = tuple(range(16))
GATHER_DIRECT = ()
SUM_DIRECT = (5,)


def z_shift(k):
    step, side = k // 2, k % 2
    step = ORDER[step]
    if step == 0:
        return 0, side
    return ((step + 1) // 2 if step % 2 else NZ - step // 2), side


SCHEDULE = [
    ("a0", 0), ("a0", 1), ("a1", 0), ("a0", 2), ("a1", 1), ("a2", 0), ("a1", 2), ("a2", 1),
    ("a0", 3), ("a3", 0), ("a2", 2), ("a0", 4), ("a3", 1), ("a1", 3), ("c", 0), ("a0", 5),
    ("a3", 2), ("a1", 4), ("a2", 3), ("c", 1), ("a1", 5), ("h1", 0), ("c", 2), ("a2", 4),
    ("a3", 3), ("a2", 5), ("h1", 1), ("d", 0), ("h1", 2), ("a3", 4), ("c", 3), ("a3", 5),
    ("d", 1), ("e1", 0), ("d", 2), ("c", 4), ("h1", 3), ("c", 5), ("e1", 1), ("e2", 0), ("h1", 4),
    ("e1", 2), ("d", 3), ("e2", 1), ("d", 4), ("d", 5), ("e2", 2), ("e1", 3), ("e1", 4),
    ("e2", 5), ("e2", 3), ("e2", 4),
]


NAMES = (
    ["halo", "ow", "co0", "co1", "st0", "st1", "ret"]
    + [f"down{h}{n}" for h in range(2) for n in range(3)]
    + [f"z{g}" for g in range(GROUPS)]
    + [f"{n}{g}" for g in range(GROUPS) for n in ("x0d", "x0r", "x1d", "x1r", "hd", "hr", "sd", "sr")]
)
RECV = {name: i for i, name in enumerate(NAMES)}
SENT_NAMES = (
    ["halo", "ow", "co", "st0", "st1", "ret", "down0", "down1", "z"]
    + [f"{n}{g}" for g in range(GROUPS) for n in ("x0", "x1", "h", "s")]
)
SENT = {name: i for i, name in enumerate(SENT_NAMES)}


def column_of(row_ref, size):
    eye = lax.broadcasted_iota(jnp.int32, (size, size), 0) == lax.broadcasted_iota(
        jnp.int32, (size, size), 1
    )
    row = jnp.broadcast_to(row_ref, (size, size))
    return jnp.sum(jnp.where(eye, row, 0.0), axis=1, keepdims=True)


def nt_dot(a, b, dims):
    return lax.dot_general(a, b, (dims, ((), ())), preferred_element_type=F32)


def kernel(*refs):
    away, out, near = refs[:14], refs[14], refs[15:29]
    og, ig, ci, taps, ow, res, doc, mg, fg, routes, rw, wg, wu, wdi = near
    (
        halo, co, wc, wda, wdb, wra, wrb, st, sp0, sp1, sb, x4, h4, p4, r1, r2, ob, ret, nrm,
        load_sems, sent_sems, recv_sems,
    ) = refs[29:]
    z, c = lax.axis_index("z"), lax.axis_index("c")
    y, x = lax.axis_index("y"), lax.axis_index("x")
    own = y * NX + x

    def send(src, dst, sent, recv, target):
        pltpu.make_async_remote_copy(
            src_ref=src,
            dst_ref=dst,
            send_sem=sent_sems.at[SENT[sent]],
            recv_sem=recv_sems.at[RECV[recv]],
            device_id=target,
            device_id_type=MESH_ID,
        ).start()

    def landed(like, recv):
        pltpu.make_async_remote_copy(
            src_ref=like,
            dst_ref=like,
            send_sem=sent_sems.at[0],
            recv_sem=recv_sems.at[RECV[recv]],
            device_id=(z, c, y, lax.rem(x + 1, NX)),
            device_id_type=MESH_ID,
        ).wait_recv()

    def drained(like, sent):
        pltpu.make_async_remote_copy(
            src_ref=like,
            dst_ref=like,
            send_sem=sent_sems.at[SENT[sent]],
            recv_sem=recv_sems.at[0],
            device_id=(z, c, y, lax.rem(x + 1, NX)),
            device_id_type=MESH_ID,
        ).wait_send()

    def in_plane(p):
        return lax.rem(y + p // NX, NY), lax.rem(x + p % NX, NX)

    def from_plane(p):
        return lax.rem(y + NY - p // NX, NY), lax.rem(x + NX - p % NX, NX)

    def along_z(k):
        dz, dc = z_shift(k)
        return (lax.rem(z + dz, NZ), lax.rem(c + dc, NC), y, x)

    def back_z(k):
        dz, dc = z_shift(k)
        return (lax.rem(z + NZ - dz, NZ), lax.rem(c + NC - dc, NC), y, x)

    barrier = pltpu.get_barrier_semaphore()
    with jax.named_scope("signals"):
        for p in range(1, NY * NX):
            py, px = in_plane(p)
            pl.semaphore_signal(barrier, inc=1, device_id=(z, c, py, px), device_id_type=MESH_ID)
        for k in range(1, NSP):
            pl.semaphore_signal(barrier, inc=1, device_id=along_z(k), device_id_type=MESH_ID)

    loads = [
        pltpu.make_async_copy(far, here, load_sems.at[i])
        for i, (far, here) in enumerate(zip(away, near))
    ]
    for i in (9, 1, 2, 6, 3, 4, 0, 5, 7, 8, 10, 13, 11, 12):
        loads[i].start()

    with jax.named_scope("local"):
        for i in range(11):
            loads[i].wait()
        product = ig[...].astype(F32) * ci[...].astype(F32)
        marks = doc[...].astype(F32)
        halo[0, 0:32, :] = product[:, 128:256]
        halo[0, 32:40, :] = jnp.broadcast_to(marks[:, 128:256], (8, 128))
        tap = [column_of(taps[i : i + 1, :], 32) for i in range(3)]
        ids = lax.broadcasted_iota(jnp.int32, (NSP, 256), 0)
        hits = [(routes[i : i + 1, :] == ids).astype(F32) for i in range(2)]
        before = (
            lax.broadcasted_iota(jnp.int32, (256, 256), 0)
            < lax.broadcasted_iota(jnp.int32, (256, 256), 1)
        ).astype(F32)
        counts = jnp.dot(
            (hits[0] + hits[1]).astype(BF), before.astype(BF), preferred_element_type=F32
        )
        slots = lax.broadcasted_iota(jnp.int32, (ROWS, 256), 0)
        for i, chosen in ((0, sp0), (1, sp1)):
            rank = jnp.sum(hits[i] * counts, axis=0, keepdims=True).astype(jnp.int32)
            expert = routes[i : i + 1, :]
            ez = jnp.right_shift(expert, 1)
            ec = expert - 2 * ez
            dz = ez - z
            dz = jnp.where(dz < 0, dz + NZ, dz)
            dc = jnp.where(ec == c, 0, 1)
            step = jnp.where(dz == 0, 0, jnp.where(dz <= NZ // 2, 2 * dz - 1, 2 * (NZ - dz)))
            place = jnp.zeros_like(step)
            for here, there in enumerate(ORDER):
                place = jnp.where(step == there, here, place)
            step = place
            slot = (step * 2 + dc) * CAP + rank
            chosen[...] = jnp.where(slots == slot, 1.0, 0.0).astype(BF)

    with jax.named_scope("entry"):
        pl.semaphore_wait(barrier, NY * NX - 1 + NSP - 1)

    my_rows = pl.ds(pl.multiple_of(own * 32, 32), 32)

    def mix(before, before_mark, piece, mark):
        lanes = lax.broadcasted_iota(jnp.int32, (32, 128), 1)
        lane_row = lax.broadcasted_iota(jnp.int32, (1, 128), 1)
        mixed = tap[2] * piece
        for shift in (1, 2):
            back = jnp.where(
                lanes < shift, pltpu.roll(before, shift, 1), pltpu.roll(piece, shift, 1)
            )
            back_mark = jnp.where(
                lane_row < shift, pltpu.roll(before_mark, shift, 1), pltpu.roll(mark, shift, 1)
            )
            same = jnp.where(back_mark == mark, 1.0, 0.0)
            mixed = mixed + (same * tap[2 - shift]) * back
        return mixed

    def send_mixed(part):
        cols = pl.ds(part * 128, 128)
        for p in range(1, NY * NX):
            py, px = in_plane(p)
            send(co.at[my_rows, cols], co.at[my_rows, cols], "co", f"co{part}", (z, c, py, px))

    with jax.named_scope("halo_send"):
        send(halo.at[0], halo.at[1], "halo", "halo", (lax.rem(z + c, NZ), 1 - c, y, x))
        late = mix(product[:, 0:128], marks[:, 0:128], product[:, 128:256], marks[:, 128:256])
        co[my_rows, 128:256] = (og[:, 128:256].astype(F32) * late).astype(BF)
        send_mixed(1)
        for p in range(1, NY * NX):
            py, px = in_plane(p)
            there = py * NX + px
            send(
                ow.at[:, pl.ds(pl.multiple_of(there * 128, 128), 128)], wc.at[my_rows, :],
                "ow", "ow", (z, c, py, px),
            )
        wc[my_rows, :] = ow[:, pl.ds(pl.multiple_of(own * 128, 128), 128)]
    with jax.named_scope("halo_wait"):
        landed(halo.at[1], "halo")
    with jax.named_scope("conv"):
        first = jnp.where((z == 0) & (c == 0), 1.0, 0.0)
        prior_mark = halo[1, 32:33, :] * (1.0 - first) - first
        early = mix(halo[1, 0:32, :], prior_mark, product[:, 0:128], marks[:, 0:128])
        co[my_rows, 0:128] = (og[:, 0:128].astype(F32) * early).astype(BF)
        send_mixed(0)
    with jax.named_scope("residual"):
        stream_t = ALPHA * res[...].astype(F32).T

    def ring(axis, step):
        if axis == "x":
            return (z, c, y, lax.rem(x + step + NX, NX))
        return (z, c, lax.rem(y + step + NY, NY), x)

    def spot(axis, step):
        return lax.rem((x if axis == "x" else y) + step + 4, 4)

    def down_rows(half, step, part=None):
        lead = spot("yx"[half], step)
        if half == 0:
            return wdi.at[lead] if part is None else wdi.at[lead, pl.ds(2 * part, 2)]
        return wdi.at[:, lead] if part is None else wdi.at[pl.ds(2 * part, 2), lead]

    def down_cols(half, step, part=None):
        cols = pl.ds(pl.multiple_of(spot("yx"[half], step) * 128, 128), 128)
        buf = (wda, wdb)[half]
        return buf.at[:, :, cols] if part is None else buf.at[pl.ds(2 * part, 2), :, cols]

    def down_sends():
        loads[13].wait()
        for half in range(2):
            for way in range(2):
                send(
                    down_rows(half, 2, way), (wra, wrb)[half].at[way], f"down{half}",
                    f"down{half}0", ring("yx"[half], 1 - 2 * way),
                )
        for half in range(2):
            for way in range(2):
                step = 1 - 2 * way
                send(
                    down_rows(half, step), down_cols(half, 0), f"down{half}", f"down{half}1",
                    ring("yx"[half], step),
                )
        own_y = pl.ds(pl.multiple_of(y * 128, 128), 128)
        own_x = pl.ds(pl.multiple_of(x * 128, 128), 128)
        wda[:, :, own_y] = wdi[y]
        wdb[:, :, own_x] = wdi[:, x]

    def down_relay():
        for half in range(2):
            landed((wra, wrb)[half], f"down{half}0")
            for way in range(2):
                step = 1 - 2 * way
                send(
                    (wra, wrb)[half].at[way], down_cols(half, -step, way), f"down{half}",
                    f"down{half}2", ring("yx"[half], step),
                )

    def down_end():
        for half in range(2):
            buf = (wda, wdb)[half]
            landed(buf.at[:, :, pl.ds(0, 256)], f"down{half}1")
            landed(buf.at[:, :, pl.ds(0, 128)], f"down{half}2")

    with jax.named_scope("mix_wait"):
        landed(wc.at[pl.ds(0, 480), :], "ow")
        landed(co.at[pl.ds(0, 480), pl.ds(0, 128)], "co1")
        landed(co.at[pl.ds(0, 480), pl.ds(0, 128)], "co0")
    with jax.named_scope("mix_dot"):
        stream_t = stream_t + nt_dot(wc[...], co[...], ((0,), (0,)))

    def norm(stream, which, gain_col):
        s1 = jnp.sum(stream, axis=0, keepdims=True)
        s2 = jnp.sum(stream * stream, axis=0, keepdims=True)
        sub = lax.broadcasted_iota(jnp.int32, (2, 256), 0)
        st[which, own] = jnp.where(sub == 0, s1, s2)
        for p in range(1, NY * NX):
            py, px = in_plane(p)
            send(st.at[which, own], st.at[which, own], f"st{which}", f"st{which}", (z, c, py, px))
        if which == 0:
            down_sends()
        landed(st.at[which, pl.ds(0, 15)], f"st{which}")
        total = st[which, 0]
        for j in range(1, NY * NX):
            total = total + st[which, j]
        mean = total[0:1, :] / D
        spread = total[1:2, :] / D - mean * mean
        return (stream - mean) * lax.rsqrt(spread + EPSILON) * gain_col

    with jax.named_scope("norm_a"):
        normed_t = norm(stream_t, 0, column_of(mg[...], 128)).astype(BF)
    nrm[...] = normed_t

    def rows_of(g):
        return pl.ds(STARTS[g] * 64, SIZES[g] * 64)

    def ks_of(g):
        return range(STARTS[g] * 2, (STARTS[g] + SIZES[g]) * 2)

    with jax.named_scope("dispatch"):
        for g in range(GROUPS):
            rows = rows_of(g)
            chosen = sp0[rows, :] + sp1[rows, :]
            sb[rows, :] = nt_dot(chosen, normed_t, ((1,), (1,))).astype(BF)
            for k in ks_of(g):
                cut = pl.ds(k * CAP, CAP)
                if k == 0:
                    x4[y, x, cut, :] = sb[cut, :]
                else:
                    send(sb.at[cut, :], x4.at[y, x, cut, :], "z", f"z{g}", along_z(k))
    with jax.named_scope("down_relay"):
        down_relay()

    def span(g, half, part):
        length = SIZES[g] * 32
        start = STARTS[g] * 64 + half * length
        if part == "lo":
            return pl.ds(start, length // 2)
        if part == "hi":
            return pl.ds(start + length // 2, length // 2)
        return pl.ds(start, length)

    def slab(buf, g, half, phase, step, part=None):
        rows = span(g, half, part)
        if half == 0:
            if phase == 0:
                return buf.at[y, spot("x", step), rows, :]
            return buf.at[spot("y", step), :, rows, :]
        if phase == 0:
            return buf.at[spot("y", step), x, rows, :]
        return buf.at[:, spot("x", step), rows, :]

    def axis_of(half, phase):
        return "xy"[(half + phase) % 2]

    def steps_of(g, chosen):
        return (1, -1, 2) if g in chosen else (1, -1)

    def ag_like(g, phase, count):
        if phase == 0:
            return x4.at[0, pl.ds(0, count), rows_of(g), :]
        return x4.at[pl.ds(0, count), :, rows_of(g), :]

    def ag_send(g, phase):
        for half in range(2):
            for step in steps_of(g, GATHER_DIRECT):
                mine = slab(x4, g, half, phase, 0)
                send(mine, mine, f"x{phase}{g}", f"x{phase}d{g}", ring(axis_of(half, phase), step))

    def ag_relay(g, phase):
        landed(ag_like(g, phase, 2), f"x{phase}d{g}")
        for half in range(2):
            for step, part in ((1, "lo"), (-1, "hi")):
                piece = slab(x4, g, half, phase, -step, part)
                send(
                    piece, piece, f"x{phase}{g}", f"x{phase}r{g}", ring(axis_of(half, phase), step)
                )

    def ag_end(g, phase):
        if g in GATHER_DIRECT:
            landed(ag_like(g, phase, 3), f"x{phase}d{g}")
        else:
            landed(ag_like(g, phase, 1), f"x{phase}r{g}")

    def expert_in(g):
        rows = rows_of(g)
        inputs = jnp.concatenate(
            [x4[b, a, rows, :] for b in range(NY) for a in range(NX)], axis=1
        )
        gate = jnp.minimum(jnp.dot(inputs, wg[...], preferred_element_type=F32), LIMIT)
        up = jnp.clip(jnp.dot(inputs, wu[...], preferred_element_type=F32), -LIMIT, LIMIT)
        hidden = ((up + 1.0) * gate * jax.nn.sigmoid(SLOPE * gate)).astype(BF)
        for half in range(2):
            h4[spot("xy"[half], 0), span(g, half, None), :] = hidden[
                half * SIZES[g] * 32 : (half + 1) * SIZES[g] * 32, :
            ]

    def hidden_at(g, half, step, part=None):
        return h4.at[spot("xy"[half], step), span(g, half, part), :]

    def hidden_send(g):
        for half in range(2):
            for step in steps_of(g, SUM_DIRECT):
                mine = hidden_at(g, half, 0)
                send(mine, mine, f"h{g}", f"hd{g}", ring("xy"[half], step))

    def hidden_relay(g):
        landed(h4.at[pl.ds(0, 2), rows_of(g), :], f"hd{g}")
        for half in range(2):
            for step, part in ((1, "lo"), (-1, "hi")):
                piece = hidden_at(g, half, -step, part)
                send(piece, piece, f"h{g}", f"hr{g}", ring("xy"[half], step))

    def hidden_end(g):
        if g in SUM_DIRECT:
            landed(h4.at[pl.ds(0, 3), rows_of(g), :], f"hd{g}")
        else:
            landed(h4.at[pl.ds(0, 1), rows_of(g), :], f"hr{g}")

    def expert_out(g):
        for half in range(2):
            rows = span(g, half, None)
            inputs = jnp.concatenate([h4[b, rows, :] for b in range(4)], axis=1)
            weights = (wda, wdb)[half][...].reshape(1024, 512)
            part = jnp.dot(inputs, weights, preferred_element_type=F32).astype(BF)
            for b in range(4):
                p4[b, rows, :] = part[:, b * 128 : (b + 1) * 128]

    def part_at(g, half, step, part=None):
        return p4.at[spot("yx"[half], step), span(g, half, part), :]

    def first_at(g, half, way):
        return r1.at[half, way, pl.ds(STARTS[g] * 16, SIZES[g] * 16), :]

    def second_at(g, half, way):
        return r2.at[half, way, pl.ds(STARTS[g] * 32, SIZES[g] * 32), :]

    def sum_first(g):
        for half in range(2):
            axis = "yx"[half]
            if g in SUM_DIRECT:
                for way, step in enumerate(steps_of(g, SUM_DIRECT)):
                    send(
                        part_at(g, half, step), second_at(g, half, way), f"s{g}", f"sd{g}",
                        ring(axis, step),
                    )
            else:
                for way, part in ((0, "lo"), (1, "hi")):
                    send(
                        part_at(g, half, 2, part), first_at(g, half, way), f"s{g}", f"sr{g}",
                        ring(axis, 1 - 2 * way),
                    )

    def sum_second(g):
        landed(p4.at[pl.ds(0, 1), rows_of(g), :], f"sr{g}")
        for half in range(2):
            for way, part in ((0, "lo"), (1, "hi")):
                step = 1 - 2 * way
                edge = part_at(g, half, step, part)
                came = first_at(g, half, way)
                edge[...] = (edge[...].astype(F32) + came[...].astype(F32)).astype(BF)
                send(
                    part_at(g, half, step), second_at(g, half, way), f"s{g}", f"sd{g}",
                    ring("yx"[half], step),
                )

    def sum_end(g):
        ways = len(steps_of(g, SUM_DIRECT))
        landed(p4.at[pl.ds(0, ways), rows_of(g), :], f"sd{g}")
        for half in range(2):
            total = part_at(g, half, 0)[...].astype(F32)
            for way in range(ways):
                total = total + second_at(g, half, way)[...].astype(F32)
            ob[span(g, half, None), :] = total.astype(BF)

    for stage, g in SCHEDULE:
        with jax.named_scope(f"{stage}_{g}"):
            if stage == "a0":
                skip = CAP if g == 0 else 0
                arrived = pl.ds(STARTS[g] * 64 + skip, SIZES[g] * 64 - skip)
                landed(x4.at[y, x, arrived, :], f"z{g}")
                ag_send(g, 0)
            elif stage == "a1":
                ag_relay(g, 0)
            elif stage == "a2":
                ag_end(g, 0)
                ag_send(g, 1)
            elif stage == "a3":
                ag_relay(g, 1)
            elif stage == "c":
                ag_end(g, 1)
                if g == 0:
                    loads[11].wait()
                    loads[12].wait()
                expert_in(g)
                hidden_send(g)
            elif stage == "h1":
                hidden_relay(g)
            elif stage == "d":
                hidden_end(g)
                if g == 0:
                    down_end()
                expert_out(g)
                sum_first(g)
            elif stage == "e1":
                sum_second(g)
            else:
                sum_end(g)
                for k in ks_of(g):
                    cut = pl.ds(k * CAP, CAP)
                    if k == 0:
                        ret[cut, :] = ob[cut, :]
                    else:
                        send(ob.at[cut, :], ret.at[cut, :], "ret", "ret", back_z(k))

    with jax.named_scope("drain"):
        drained(halo.at[0], "halo")
        drained(wc.at[pl.ds(0, 480), :], "ow")
        drained(co.at[pl.ds(0, 480), :], "co")
        drained(st.at[0, pl.ds(0, 15)], "st0")
        drained(wda, "down0")
        drained(wdb, "down1")
        drained(sb.at[pl.ds(CAP, ROWS - CAP), :], "z")
        for g in range(GROUPS):
            drained(ag_like(g, 0, 3), f"x0{g}")
            drained(ag_like(g, 1, 3), f"x1{g}")
            drained(h4.at[pl.ds(0, 3), rows_of(g), :], f"h{g}")
            drained(p4.at[pl.ds(0, 3), rows_of(g), :], f"s{g}")
    with jax.named_scope("ret_wait"):
        landed(ret.at[pl.ds(CAP, ROWS - CAP), :], "ret")
    with jax.named_scope("combine"):
        results = ret[...]
        ffn = rw[0:1, :] * nt_dot(results, sp0[...], ((0,), (0,)))
        ffn = ffn + rw[1:2, :] * nt_dot(results, sp1[...], ((0,), (0,)))
        second = ALPHA * nrm[...].astype(F32) + ffn
    with jax.named_scope("norm_b"):
        out[...] = norm(second, 1, column_of(fg[...], 128)).T.astype(BF)
    drained(st.at[1, pl.ds(0, 15)], "st1")
    drained(ob.at[pl.ds(CAP, ROWS - CAP), :], "ret")


def per_device(
    out_gate, in_gate, conv_input, conv_taps, out_weight, residual, document, mix_gain,
    ffn_gain, routes, route_weight, expert_gate, expert_up, expert_down,
):
    args = (
        out_gate.T, in_gate.T, conv_input.T, conv_taps, out_weight, residual,
        document[None, :], mix_gain[None, :], ffn_gain[None, :], routes.T, route_weight.T,
        expert_gate[0], expert_up[0], expert_down[0].reshape(NY, NX, 256, 128),
    )
    dma = pltpu.SemaphoreType.DMA
    scratch = [pltpu.VMEM(arg.shape, arg.dtype) for arg in args] + [
        pltpu.VMEM((2, 40, 128), F32),
        pltpu.VMEM((512, 256), BF),
        pltpu.VMEM((512, 128), BF),
        pltpu.VMEM((4, 256, 512), BF),
        pltpu.VMEM((4, 256, 512), BF),
        pltpu.VMEM((2, 2, 256, 128), BF),
        pltpu.VMEM((2, 2, 256, 128), BF),
        pltpu.VMEM((2, 16, 2, 256), F32),
        pltpu.VMEM((ROWS, 256), BF),
        pltpu.VMEM((ROWS, 256), BF),
        pltpu.VMEM((ROWS, 128), BF),
        pltpu.VMEM((NY, NX, ROWS, 128), BF),
        pltpu.VMEM((4, ROWS, 256), BF),
        pltpu.VMEM((4, ROWS, 128), BF),
        pltpu.VMEM((2, 2, ROWS // 4, 128), BF),
        pltpu.VMEM((2, 3, ROWS // 2, 128), BF),
        pltpu.VMEM((ROWS, 128), BF),
        pltpu.VMEM((ROWS, 128), BF),
        pltpu.VMEM((128, 256), BF),
        dma((len(args),)),
        dma((len(SENT),)),
        dma((len(RECV),)),
    ]
    return pl.pallas_call(
        kernel,
        out_shape=jax.ShapeDtypeStruct((256, 128), BF),
        in_specs=[pl.BlockSpec(memory_space=pl.ANY)] * len(args),
        out_specs=pl.BlockSpec(memory_space=pltpu.VMEM),
        scratch_shapes=scratch,
        compiler_params=pltpu.CompilerParams(
            collective_id=0, has_side_effects=True, vmem_limit_bytes=60 * 1024 * 1024
        ),
    )(*args)


def solution(mesh):
    torus = Mesh(mesh.devices.reshape(NZ, NC, NY, NX), ("z", "c", "y", "x"))
    sp, tp = ("z", "c"), ("y", "x")
    in_specs = (
        P(sp, tp), P(sp, tp), P(sp, tp), P(None, tp), P(tp, None), P(sp, tp), P(sp), P(tp),
        P(tp), P(sp, None), P(sp, None), P(sp, None, tp), P(sp, None, tp), P(sp, None, tp),
    )
    return jax.shard_map(
        per_device, mesh=torus, in_specs=in_specs, out_specs=P(sp, tp), check_vma=False
    )
```

```python
import jax
import jax.numpy as jnp
from jax import lax
from jax.experimental import pallas as pl
from jax.experimental.pallas import tpu as pltpu
from jax.sharding import Mesh
from jax.sharding import PartitionSpec as P

D = 2048
CAP = 32
ALPHA = 8.0**0.25
EPSILON = 1e-05
LIMIT = 7.0
SLOPE = 1.702
MESH_ID = pl.DeviceIdType.MESH
BF = jnp.bfloat16
F32 = jnp.float32

NZ, NC, NY, NX = 16, 2, 4, 4
NSP = NZ * NC
ROWS = NSP * CAP
SIZES = (1, 1, 2, 3, 3, 3, 2, 1)
GROUPS = len(SIZES)
STARTS = tuple(sum(SIZES[:g]) for g in range(GROUPS))
ORDER = tuple(range(16))
GATHER_DIRECT = (0,)
SUM_DIRECT = (6, 7)


def z_shift(k):
    step, side = k // 2, k % 2
    step = ORDER[step]
    if step == 0:
        return 0, side
    return ((step + 1) // 2 if step % 2 else NZ - step // 2), side


SCHEDULE = [
    ("a0", 0), ("a0", 1), ("a0", 2), ("a0", 3), ("a1", 1), ("a1", 2), ("a2", 0), ("a0", 4),
    ("a1", 3), ("a2", 2), ("a2", 1), ("a0", 5), ("a1", 4), ("a2", 3), ("c", 0), ("a0", 6),
    ("a3", 2), ("a1", 5), ("a3", 1), ("a2", 4), ("a0", 7), ("a1", 6), ("h1", 0), ("a3", 3),
    ("c", 2), ("a2", 5), ("c", 1), ("a1", 7), ("a3", 4), ("a2", 6), ("d", 0), ("c", 3), ("h1", 2),
    ("a3", 5), ("h1", 1), ("a2", 7), ("c", 4), ("a3", 6), ("e1", 0), ("h1", 3), ("d", 2),
    ("c", 5), ("d", 1), ("a3", 7), ("h1", 4), ("c", 6), ("e2", 0), ("e1", 2), ("d", 3), ("h1", 5),
    ("c", 7), ("e1", 1), ("d", 4), ("e2", 2), ("e1", 3), ("d", 6), ("d", 5), ("e2", 1), ("e1", 4),
    ("d", 7), ("e2", 3), ("e1", 5), ("e2", 6), ("e2", 4), ("e2", 7), ("e2", 5),
]


NAMES = (
    ["halo", "ow", "co0", "co1", "st0", "st1", "ret"]
    + [f"down{h}{n}" for h in range(2) for n in range(3)]
    + [f"z{g}" for g in range(GROUPS)]
    + [f"{n}{g}" for g in range(GROUPS) for n in ("x0d", "x0r", "x1d", "x1r", "hd", "hr", "sd", "sr")]
)
RECV = {name: i for i, name in enumerate(NAMES)}
SENT_NAMES = (
    ["halo", "ow", "co", "st0", "st1", "ret", "down0", "down1", "z"]
    + [f"{n}{g}" for g in range(GROUPS) for n in ("x0", "x1", "h", "s")]
)
SENT = {name: i for i, name in enumerate(SENT_NAMES)}


def column_of(row_ref, size):
    eye = lax.broadcasted_iota(jnp.int32, (size, size), 0) == lax.broadcasted_iota(
        jnp.int32, (size, size), 1
    )
    row = jnp.broadcast_to(row_ref, (size, size))
    return jnp.sum(jnp.where(eye, row, 0.0), axis=1, keepdims=True)


def nt_dot(a, b, dims):
    return lax.dot_general(a, b, (dims, ((), ())), preferred_element_type=F32)


def kernel(*refs):
    away, out, near = refs[:14], refs[14], refs[15:29]
    og, ig, ci, taps, ow, res, doc, mg, fg, routes, rw, wg, wu, wdi = near
    (
        halo, co, wc, wda, wdb, wra, wrb, st, sp0, sp1, sb, x4, h4, p4, r1, r2, ob, ret, nrm,
        load_sems, sent_sems, recv_sems,
    ) = refs[29:]
    z, c = lax.axis_index("z"), lax.axis_index("c")
    y, x = lax.axis_index("y"), lax.axis_index("x")
    own = y * NX + x

    def send(src, dst, sent, recv, target):
        pltpu.make_async_remote_copy(
            src_ref=src,
            dst_ref=dst,
            send_sem=sent_sems.at[SENT[sent]],
            recv_sem=recv_sems.at[RECV[recv]],
            device_id=target,
            device_id_type=MESH_ID,
        ).start()

    def landed(like, recv):
        pltpu.make_async_remote_copy(
            src_ref=like,
            dst_ref=like,
            send_sem=sent_sems.at[0],
            recv_sem=recv_sems.at[RECV[recv]],
            device_id=(z, c, y, lax.rem(x + 1, NX)),
            device_id_type=MESH_ID,
        ).wait_recv()

    def drained(like, sent):
        pltpu.make_async_remote_copy(
            src_ref=like,
            dst_ref=like,
            send_sem=sent_sems.at[SENT[sent]],
            recv_sem=recv_sems.at[0],
            device_id=(z, c, y, lax.rem(x + 1, NX)),
            device_id_type=MESH_ID,
        ).wait_send()

    def in_plane(p):
        return lax.rem(y + p // NX, NY), lax.rem(x + p % NX, NX)

    def from_plane(p):
        return lax.rem(y + NY - p // NX, NY), lax.rem(x + NX - p % NX, NX)

    def along_z(k):
        dz, dc = z_shift(k)
        return (lax.rem(z + dz, NZ), lax.rem(c + dc, NC), y, x)

    def back_z(k):
        dz, dc = z_shift(k)
        return (lax.rem(z + NZ - dz, NZ), lax.rem(c + NC - dc, NC), y, x)

    barrier = pltpu.get_barrier_semaphore()
    with jax.named_scope("signals"):
        for p in range(1, NY * NX):
            py, px = in_plane(p)
            pl.semaphore_signal(barrier, inc=1, device_id=(z, c, py, px), device_id_type=MESH_ID)
        for k in range(1, NSP):
            pl.semaphore_signal(barrier, inc=1, device_id=along_z(k), device_id_type=MESH_ID)

    loads = [
        pltpu.make_async_copy(far, here, load_sems.at[i])
        for i, (far, here) in enumerate(zip(away, near))
    ]
    for i in (9, 1, 2, 6, 3, 4, 0, 5, 7, 8, 10, 13, 11, 12):
        loads[i].start()

    with jax.named_scope("local"):
        for i in (1, 2, 6, 3, 0):
            loads[i].wait()
        product = ig[...].astype(F32) * ci[...].astype(F32)
        marks = doc[...].astype(F32)
        halo[0, 0:32, :] = product[:, 128:256]
        halo[0, 32:40, :] = jnp.broadcast_to(marks[:, 128:256], (8, 128))
        tap = [column_of(taps[i : i + 1, :], 32) for i in range(3)]

    with jax.named_scope("entry"):
        pl.semaphore_wait(barrier, NY * NX - 1 + NSP - 1)

    my_rows = pl.ds(pl.multiple_of(own * 32, 32), 32)

    def mix(before, before_mark, piece, mark):
        lanes = lax.broadcasted_iota(jnp.int32, (32, 128), 1)
        lane_row = lax.broadcasted_iota(jnp.int32, (1, 128), 1)
        mixed = tap[2] * piece
        for shift in (1, 2):
            back = jnp.where(
                lanes < shift, pltpu.roll(before, shift, 1), pltpu.roll(piece, shift, 1)
            )
            back_mark = jnp.where(
                lane_row < shift, pltpu.roll(before_mark, shift, 1), pltpu.roll(mark, shift, 1)
            )
            same = jnp.where(back_mark == mark, 1.0, 0.0)
            mixed = mixed + (same * tap[2 - shift]) * back
        return mixed

    def send_mixed(part):
        cols = pl.ds(part * 128, 128)
        for p in range(1, NY * NX):
            py, px = in_plane(p)
            send(co.at[my_rows, cols], co.at[my_rows, cols], "co", f"co{part}", (z, c, py, px))

    with jax.named_scope("halo_send"):
        send(halo.at[0], halo.at[1], "halo", "halo", (lax.rem(z + c, NZ), 1 - c, y, x))
        late = mix(product[:, 0:128], marks[:, 0:128], product[:, 128:256], marks[:, 128:256])
        co[my_rows, 128:256] = (og[:, 128:256].astype(F32) * late).astype(BF)
        send_mixed(1)
        loads[4].wait()
        for p in range(1, NY * NX):
            py, px = in_plane(p)
            there = py * NX + px
            send(
                ow.at[:, pl.ds(pl.multiple_of(there * 128, 128), 128)], wc.at[my_rows, :],
                "ow", "ow", (z, c, py, px),
            )
        wc[my_rows, :] = ow[:, pl.ds(pl.multiple_of(own * 128, 128), 128)]
    with jax.named_scope("halo_wait"):
        landed(halo.at[1], "halo")
    with jax.named_scope("conv"):
        first = jnp.where((z == 0) & (c == 0), 1.0, 0.0)
        prior_mark = halo[1, 32:33, :] * (1.0 - first) - first
        early = mix(halo[1, 0:32, :], prior_mark, product[:, 0:128], marks[:, 0:128])
        co[my_rows, 0:128] = (og[:, 0:128].astype(F32) * early).astype(BF)
        send_mixed(0)
    with jax.named_scope("slots"):
        for i in (5, 7, 8, 9, 10):
            loads[i].wait()
        ids = lax.broadcasted_iota(jnp.int32, (NSP, 256), 0)
        hits = [(routes[i : i + 1, :] == ids).astype(F32) for i in range(2)]
        before = (
            lax.broadcasted_iota(jnp.int32, (256, 256), 0)
            < lax.broadcasted_iota(jnp.int32, (256, 256), 1)
        ).astype(F32)
        counts = jnp.dot(
            (hits[0] + hits[1]).astype(BF), before.astype(BF), preferred_element_type=F32
        )
        slots = lax.broadcasted_iota(jnp.int32, (ROWS, 256), 0)
        for i, chosen in ((0, sp0), (1, sp1)):
            rank = jnp.sum(hits[i] * counts, axis=0, keepdims=True).astype(jnp.int32)
            expert = routes[i : i + 1, :]
            ez = jnp.right_shift(expert, 1)
            ec = expert - 2 * ez
            dz = ez - z
            dz = jnp.where(dz < 0, dz + NZ, dz)
            dc = jnp.where(ec == c, 0, 1)
            step = jnp.where(dz == 0, 0, jnp.where(dz <= NZ // 2, 2 * dz - 1, 2 * (NZ - dz)))
            place = jnp.zeros_like(step)
            for here, there in enumerate(ORDER):
                place = jnp.where(step == there, here, place)
            step = place
            slot = (step * 2 + dc) * CAP + rank
            chosen[...] = jnp.where(slots == slot, 1.0, 0.0).astype(BF)
    with jax.named_scope("residual"):
        stream_t = ALPHA * res[...].astype(F32).T

    def ring(axis, step):
        if axis == "x":
            return (z, c, y, lax.rem(x + step + NX, NX))
        return (z, c, lax.rem(y + step + NY, NY), x)

    def spot(axis, step):
        return lax.rem((x if axis == "x" else y) + step + 4, 4)

    def down_rows(half, step, part=None):
        lead = spot("yx"[half], step)
        if half == 0:
            return wdi.at[lead] if part is None else wdi.at[lead, pl.ds(2 * part, 2)]
        return wdi.at[:, lead] if part is None else wdi.at[pl.ds(2 * part, 2), lead]

    def down_cols(half, step, part=None):
        cols = pl.ds(pl.multiple_of(spot("yx"[half], step) * 128, 128), 128)
        buf = (wda, wdb)[half]
        return buf.at[:, :, cols] if part is None else buf.at[pl.ds(2 * part, 2), :, cols]

    def down_sends():
        loads[13].wait()
        for half in range(2):
            for way in range(2):
                send(
                    down_rows(half, 2, way), (wra, wrb)[half].at[way], f"down{half}",
                    f"down{half}0", ring("yx"[half], 1 - 2 * way),
                )
        for half in range(2):
            for way in range(2):
                step = 1 - 2 * way
                send(
                    down_rows(half, step), down_cols(half, 0), f"down{half}", f"down{half}1",
                    ring("yx"[half], step),
                )
        own_y = pl.ds(pl.multiple_of(y * 128, 128), 128)
        own_x = pl.ds(pl.multiple_of(x * 128, 128), 128)
        wda[:, :, own_y] = wdi[y]
        wdb[:, :, own_x] = wdi[:, x]

    def down_relay():
        for half in range(2):
            landed((wra, wrb)[half], f"down{half}0")
            for way in range(2):
                step = 1 - 2 * way
                send(
                    (wra, wrb)[half].at[way], down_cols(half, -step, way), f"down{half}",
                    f"down{half}2", ring("yx"[half], step),
                )

    def down_end():
        for half in range(2):
            buf = (wda, wdb)[half]
            landed(buf.at[:, :, pl.ds(0, 256)], f"down{half}1")
            landed(buf.at[:, :, pl.ds(0, 128)], f"down{half}2")

    with jax.named_scope("mix_wait"):
        landed(wc.at[pl.ds(0, 480), :], "ow")
        landed(co.at[pl.ds(0, 480), pl.ds(0, 128)], "co1")
        landed(co.at[pl.ds(0, 480), pl.ds(0, 128)], "co0")
    with jax.named_scope("mix_dot"):
        stream_t = stream_t + nt_dot(wc[...], co[...], ((0,), (0,)))

    def norm(stream, which, gain_col):
        s1 = jnp.sum(stream, axis=0, keepdims=True)
        s2 = jnp.sum(stream * stream, axis=0, keepdims=True)
        sub = lax.broadcasted_iota(jnp.int32, (2, 256), 0)
        st[which, own] = jnp.where(sub == 0, s1, s2)
        for p in range(1, NY * NX):
            py, px = in_plane(p)
            send(st.at[which, own], st.at[which, own], f"st{which}", f"st{which}", (z, c, py, px))
        if which == 0:
            down_sends()
        landed(st.at[which, pl.ds(0, 15)], f"st{which}")
        total = st[which, 0]
        for j in range(1, NY * NX):
            total = total + st[which, j]
        mean = total[0:1, :] / D
        spread = total[1:2, :] / D - mean * mean
        return (stream - mean) * lax.rsqrt(spread + EPSILON) * gain_col

    with jax.named_scope("norm_a"):
        normed_t = norm(stream_t, 0, column_of(mg[...], 128)).astype(BF)
    nrm[...] = normed_t

    def rows_of(g):
        return pl.ds(STARTS[g] * 64, SIZES[g] * 64)

    def ks_of(g):
        return range(STARTS[g] * 2, (STARTS[g] + SIZES[g]) * 2)

    with jax.named_scope("dispatch"):
        for g in range(GROUPS):
            rows = rows_of(g)
            chosen = sp0[rows, :] + sp1[rows, :]
            sb[rows, :] = nt_dot(chosen, normed_t, ((1,), (1,))).astype(BF)
            for k in ks_of(g):
                cut = pl.ds(k * CAP, CAP)
                if k == 0:
                    x4[y, x, cut, :] = sb[cut, :]
                else:
                    send(sb.at[cut, :], x4.at[y, x, cut, :], "z", f"z{g}", along_z(k))
    with jax.named_scope("down_relay"):
        down_relay()

    def span(g, half, part):
        length = SIZES[g] * 32
        start = STARTS[g] * 64 + half * length
        if part == "lo":
            return pl.ds(start, length // 2)
        if part == "hi":
            return pl.ds(start + length // 2, length // 2)
        return pl.ds(start, length)

    def slab(buf, g, half, phase, step, part=None):
        rows = span(g, half, part)
        if half == 0:
            if phase == 0:
                return buf.at[y, spot("x", step), rows, :]
            return buf.at[spot("y", step), :, rows, :]
        if phase == 0:
            return buf.at[spot("y", step), x, rows, :]
        return buf.at[:, spot("x", step), rows, :]

    def axis_of(half, phase):
        return "xy"[(half + phase) % 2]

    def steps_of(g, chosen):
        return (1, -1, 2) if g in chosen else (1, -1)

    def ag_like(g, phase, count):
        if phase == 0:
            return x4.at[0, pl.ds(0, count), rows_of(g), :]
        return x4.at[pl.ds(0, count), :, rows_of(g), :]

    def ag_send(g, phase):
        for half in range(2):
            for step in steps_of(g, GATHER_DIRECT):
                mine = slab(x4, g, half, phase, 0)
                send(mine, mine, f"x{phase}{g}", f"x{phase}d{g}", ring(axis_of(half, phase), step))

    def ag_relay(g, phase):
        landed(ag_like(g, phase, 2), f"x{phase}d{g}")
        for half in range(2):
            for step, part in ((1, "lo"), (-1, "hi")):
                piece = slab(x4, g, half, phase, -step, part)
                send(
                    piece, piece, f"x{phase}{g}", f"x{phase}r{g}", ring(axis_of(half, phase), step)
                )

    def ag_end(g, phase):
        if g in GATHER_DIRECT:
            landed(ag_like(g, phase, 3), f"x{phase}d{g}")
        else:
            landed(ag_like(g, phase, 1), f"x{phase}r{g}")

    def expert_in(g):
        rows = rows_of(g)
        inputs = jnp.concatenate(
            [x4[b, a, rows, :] for b in range(NY) for a in range(NX)], axis=1
        )
        gate = jnp.minimum(jnp.dot(inputs, wg[...], preferred_element_type=F32), LIMIT)
        up = jnp.clip(jnp.dot(inputs, wu[...], preferred_element_type=F32), -LIMIT, LIMIT)
        hidden = ((up + 1.0) * gate * jax.nn.sigmoid(SLOPE * gate)).astype(BF)
        for half in range(2):
            h4[spot("xy"[half], 0), span(g, half, None), :] = hidden[
                half * SIZES[g] * 32 : (half + 1) * SIZES[g] * 32, :
            ]

    def hidden_at(g, half, step, part=None):
        return h4.at[spot("xy"[half], step), span(g, half, part), :]

    def hidden_send(g):
        for half in range(2):
            for step in steps_of(g, SUM_DIRECT):
                mine = hidden_at(g, half, 0)
                send(mine, mine, f"h{g}", f"hd{g}", ring("xy"[half], step))

    def hidden_relay(g):
        landed(h4.at[pl.ds(0, 2), rows_of(g), :], f"hd{g}")
        for half in range(2):
            for step, part in ((1, "lo"), (-1, "hi")):
                piece = hidden_at(g, half, -step, part)
                send(piece, piece, f"h{g}", f"hr{g}", ring("xy"[half], step))

    def hidden_end(g):
        if g in SUM_DIRECT:
            landed(h4.at[pl.ds(0, 3), rows_of(g), :], f"hd{g}")
        else:
            landed(h4.at[pl.ds(0, 1), rows_of(g), :], f"hr{g}")

    def expert_out(g):
        for half in range(2):
            rows = span(g, half, None)
            inputs = jnp.concatenate([h4[b, rows, :] for b in range(4)], axis=1)
            weights = (wda, wdb)[half][...].reshape(1024, 512)
            part = jnp.dot(inputs, weights, preferred_element_type=F32).astype(BF)
            for b in range(4):
                p4[b, rows, :] = part[:, b * 128 : (b + 1) * 128]

    def part_at(g, half, step, part=None):
        return p4.at[spot("yx"[half], step), span(g, half, part), :]

    def first_at(g, half, way):
        return r1.at[half, way, pl.ds(STARTS[g] * 16, SIZES[g] * 16), :]

    def second_at(g, half, way):
        return r2.at[half, way, pl.ds(STARTS[g] * 32, SIZES[g] * 32), :]

    def sum_first(g):
        for half in range(2):
            axis = "yx"[half]
            if g in SUM_DIRECT:
                for way, step in enumerate(steps_of(g, SUM_DIRECT)):
                    send(
                        part_at(g, half, step), second_at(g, half, way), f"s{g}", f"sd{g}",
                        ring(axis, step),
                    )
            else:
                for way, part in ((0, "lo"), (1, "hi")):
                    send(
                        part_at(g, half, 2, part), first_at(g, half, way), f"s{g}", f"sr{g}",
                        ring(axis, 1 - 2 * way),
                    )

    def sum_second(g):
        landed(p4.at[pl.ds(0, 1), rows_of(g), :], f"sr{g}")
        for half in range(2):
            for way, part in ((0, "lo"), (1, "hi")):
                step = 1 - 2 * way
                edge = part_at(g, half, step, part)
                came = first_at(g, half, way)
                edge[...] = (edge[...].astype(F32) + came[...].astype(F32)).astype(BF)
                send(
                    part_at(g, half, step), second_at(g, half, way), f"s{g}", f"sd{g}",
                    ring("yx"[half], step),
                )

    def sum_end(g):
        ways = len(steps_of(g, SUM_DIRECT))
        landed(p4.at[pl.ds(0, ways), rows_of(g), :], f"sd{g}")
        for half in range(2):
            total = part_at(g, half, 0)[...].astype(F32)
            for way in range(ways):
                total = total + second_at(g, half, way)[...].astype(F32)
            ob[span(g, half, None), :] = total.astype(BF)

    for stage, g in SCHEDULE:
        with jax.named_scope(f"{stage}_{g}"):
            if stage == "a0":
                skip = CAP if g == 0 else 0
                arrived = pl.ds(STARTS[g] * 64 + skip, SIZES[g] * 64 - skip)
                landed(x4.at[y, x, arrived, :], f"z{g}")
                ag_send(g, 0)
            elif stage == "a1":
                ag_relay(g, 0)
            elif stage == "a2":
                ag_end(g, 0)
                ag_send(g, 1)
            elif stage == "a3":
                ag_relay(g, 1)
            elif stage == "c":
                ag_end(g, 1)
                if g == 0:
                    loads[11].wait()
                    loads[12].wait()
                expert_in(g)
                hidden_send(g)
            elif stage == "h1":
                hidden_relay(g)
            elif stage == "d":
                hidden_end(g)
                if g == 0:
                    down_end()
                expert_out(g)
                sum_first(g)
            elif stage == "e1":
                sum_second(g)
            else:
                sum_end(g)
                for k in ks_of(g):
                    cut = pl.ds(k * CAP, CAP)
                    if k == 0:
                        ret[cut, :] = ob[cut, :]
                    else:
                        send(ob.at[cut, :], ret.at[cut, :], "ret", "ret", back_z(k))

    with jax.named_scope("drain"):
        drained(halo.at[0], "halo")
        drained(wc.at[pl.ds(0, 480), :], "ow")
        drained(co.at[pl.ds(0, 480), :], "co")
        drained(st.at[0, pl.ds(0, 15)], "st0")
        drained(wda, "down0")
        drained(wdb, "down1")
        drained(sb.at[pl.ds(CAP, ROWS - CAP), :], "z")
        for g in range(GROUPS):
            drained(ag_like(g, 0, 3), f"x0{g}")
            drained(ag_like(g, 1, 3), f"x1{g}")
            drained(h4.at[pl.ds(0, 3), rows_of(g), :], f"h{g}")
            drained(p4.at[pl.ds(0, 3), rows_of(g), :], f"s{g}")
    with jax.named_scope("ret_wait"):
        landed(ret.at[pl.ds(CAP, ROWS - CAP), :], "ret")
    with jax.named_scope("combine"):
        results = ret[...]
        ffn = rw[0:1, :] * nt_dot(results, sp0[...], ((0,), (0,)))
        ffn = ffn + rw[1:2, :] * nt_dot(results, sp1[...], ((0,), (0,)))
        second = ALPHA * nrm[...].astype(F32) + ffn
    with jax.named_scope("norm_b"):
        out[...] = norm(second, 1, column_of(fg[...], 128)).T.astype(BF)
    drained(st.at[1, pl.ds(0, 15)], "st1")
    drained(ob.at[pl.ds(CAP, ROWS - CAP), :], "ret")


def per_device(
    out_gate, in_gate, conv_input, conv_taps, out_weight, residual, document, mix_gain,
    ffn_gain, routes, route_weight, expert_gate, expert_up, expert_down,
):
    args = (
        out_gate.T, in_gate.T, conv_input.T, conv_taps, out_weight, residual,
        document[None, :], mix_gain[None, :], ffn_gain[None, :], routes.T, route_weight.T,
        expert_gate[0], expert_up[0], expert_down[0].reshape(NY, NX, 256, 128),
    )
    args = tuple(pltpu.with_memory_space_constraint(arg, pltpu.HBM) for arg in args)
    dma = pltpu.SemaphoreType.DMA
    scratch = [pltpu.VMEM(arg.shape, arg.dtype) for arg in args] + [
        pltpu.VMEM((2, 40, 128), F32),
        pltpu.VMEM((512, 256), BF),
        pltpu.VMEM((512, 128), BF),
        pltpu.VMEM((4, 256, 512), BF),
        pltpu.VMEM((4, 256, 512), BF),
        pltpu.VMEM((2, 2, 256, 128), BF),
        pltpu.VMEM((2, 2, 256, 128), BF),
        pltpu.VMEM((2, 16, 2, 256), F32),
        pltpu.VMEM((ROWS, 256), BF),
        pltpu.VMEM((ROWS, 256), BF),
        pltpu.VMEM((ROWS, 128), BF),
        pltpu.VMEM((NY, NX, ROWS, 128), BF),
        pltpu.VMEM((4, ROWS, 256), BF),
        pltpu.VMEM((4, ROWS, 128), BF),
        pltpu.VMEM((2, 2, ROWS // 4, 128), BF),
        pltpu.VMEM((2, 3, ROWS // 2, 128), BF),
        pltpu.VMEM((ROWS, 128), BF),
        pltpu.VMEM((ROWS, 128), BF),
        pltpu.VMEM((128, 256), BF),
        dma((len(args),)),
        dma((len(SENT),)),
        dma((len(RECV),)),
    ]
    return pl.pallas_call(
        kernel,
        out_shape=jax.ShapeDtypeStruct((256, 128), BF),
        in_specs=[pl.BlockSpec(memory_space=pl.ANY)] * len(args),
        out_specs=pl.BlockSpec(memory_space=pltpu.VMEM),
        scratch_shapes=scratch,
        compiler_params=pltpu.CompilerParams(
            collective_id=0, has_side_effects=True, vmem_limit_bytes=48 * 1024 * 1024
        ),
    )(*args)


def solution(mesh):
    torus = Mesh(mesh.devices.reshape(NZ, NC, NY, NX), ("z", "c", "y", "x"))
    sp, tp = ("z", "c"), ("y", "x")
    in_specs = (
        P(sp, tp), P(sp, tp), P(sp, tp), P(None, tp), P(tp, None), P(sp, tp), P(sp), P(tp),
        P(tp), P(sp, None), P(sp, None), P(sp, None, tp), P(sp, None, tp), P(sp, None, tp),
    )
    return jax.shard_map(
        per_device, mesh=torus, in_specs=in_specs, out_specs=P(sp, tp), check_vma=False
    )
```

```python
import jax
import jax.numpy as jnp
from jax import lax
from jax.experimental import pallas as pl
from jax.experimental.pallas import tpu as pltpu
from jax.sharding import Mesh
from jax.sharding import PartitionSpec as P

D = 2048
CAP = 32
ALPHA = 8.0**0.25
EPSILON = 1e-05
LIMIT = 7.0
SLOPE = 1.702
MESH_ID = pl.DeviceIdType.MESH
BF = jnp.bfloat16
F32 = jnp.float32

NZ, NC, NY, NX = 16, 2, 4, 4
NSP = NZ * NC
ROWS = NSP * CAP
SIZES = (1, 2, 4, 4, 2, 2, 1)
GROUPS = len(SIZES)
STARTS = tuple(sum(SIZES[:g]) for g in range(GROUPS))
ORDER = tuple(range(16))
GATHER_DIRECT = (0,)
SUM_DIRECT = (5, 6)


def z_shift(k):
    step, side = k // 2, k % 2
    step = ORDER[step]
    if step == 0:
        return 0, side
    return ((step + 1) // 2 if step % 2 else NZ - step // 2), side


SCHEDULE = [
    ("a0", 1), ("a0", 0), ("a0", 2), ("a1", 1), ("a2", 0), ("a1", 2), ("a0", 4), ("a0", 3),
    ("a2", 2), ("a0", 5), ("a1", 4), ("a1", 3), ("a0", 6), ("a1", 5), ("a2", 4), ("a2", 3),
    ("a2", 1), ("a1", 6), ("a2", 5), ("a3", 2), ("a3", 4), ("c", 0), ("a2", 6), ("a3", 5),
    ("a3", 3), ("a3", 1), ("a3", 6), ("c", 4), ("c", 5), ("c", 3), ("h1", 4), ("c", 6), ("c", 2),
    ("h1", 3), ("d", 5), ("c", 1), ("d", 4), ("h1", 2), ("d", 6), ("h1", 0), ("d", 3), ("h1", 1),
    ("e2", 5), ("e1", 4), ("d", 2), ("d", 0), ("e2", 6), ("e1", 3), ("d", 1), ("e2", 4),
    ("e1", 2), ("e2", 3), ("e1", 0), ("e1", 1), ("e2", 2), ("e2", 0), ("e2", 1),
]


NAMES = (
    ["halo", "ow", "co0", "co1", "st0", "st1", "ret"]
    + [f"down{h}{n}" for h in range(2) for n in range(3)]
    + [f"z{g}" for g in range(GROUPS)]
    + [f"{n}{g}" for g in range(GROUPS) for n in ("x0d", "x0r", "x1d", "x1r", "hd", "hr", "sd", "sr")]
)
RECV = {name: i for i, name in enumerate(NAMES)}
SENT_NAMES = (
    ["halo", "ow", "co", "st0", "st1", "ret", "down0", "down1", "z"]
    + [f"{n}{g}" for g in range(GROUPS) for n in ("x0", "x1", "h", "s")]
)
SENT = {name: i for i, name in enumerate(SENT_NAMES)}


def column_of(row_ref, size):
    eye = lax.broadcasted_iota(jnp.int32, (size, size), 0) == lax.broadcasted_iota(
        jnp.int32, (size, size), 1
    )
    row = jnp.broadcast_to(row_ref, (size, size))
    return jnp.sum(jnp.where(eye, row, 0.0), axis=1, keepdims=True)


def nt_dot(a, b, dims):
    return lax.dot_general(a, b, (dims, ((), ())), preferred_element_type=F32)


def kernel(*refs):
    away, out, near = refs[:14], refs[14], refs[15:29]
    og, ig, ci, taps, ow, res, doc, mg, fg, routes, rw, wg, wu, wdi = near
    (
        halo, co, wc, wda, wdb, wra, wrb, st, sp0, sp1, sb, x4, h4, p4, r1, r2, ob, ret, nrm,
        load_sems, sent_sems, recv_sems,
    ) = refs[29:]
    z, c = lax.axis_index("z"), lax.axis_index("c")
    y, x = lax.axis_index("y"), lax.axis_index("x")
    own = y * NX + x

    def send(src, dst, sent, recv, target):
        pltpu.make_async_remote_copy(
            src_ref=src,
            dst_ref=dst,
            send_sem=sent_sems.at[SENT[sent]],
            recv_sem=recv_sems.at[RECV[recv]],
            device_id=target,
            device_id_type=MESH_ID,
        ).start()

    def landed(like, recv):
        pltpu.make_async_remote_copy(
            src_ref=like,
            dst_ref=like,
            send_sem=sent_sems.at[0],
            recv_sem=recv_sems.at[RECV[recv]],
            device_id=(z, c, y, lax.rem(x + 1, NX)),
            device_id_type=MESH_ID,
        ).wait_recv()

    def drained(like, sent):
        pltpu.make_async_remote_copy(
            src_ref=like,
            dst_ref=like,
            send_sem=sent_sems.at[SENT[sent]],
            recv_sem=recv_sems.at[0],
            device_id=(z, c, y, lax.rem(x + 1, NX)),
            device_id_type=MESH_ID,
        ).wait_send()

    def in_plane(p):
        return lax.rem(y + p // NX, NY), lax.rem(x + p % NX, NX)

    def from_plane(p):
        return lax.rem(y + NY - p // NX, NY), lax.rem(x + NX - p % NX, NX)

    def along_z(k):
        dz, dc = z_shift(k)
        return (lax.rem(z + dz, NZ), lax.rem(c + dc, NC), y, x)

    def back_z(k):
        dz, dc = z_shift(k)
        return (lax.rem(z + NZ - dz, NZ), lax.rem(c + NC - dc, NC), y, x)

    barrier = pltpu.get_barrier_semaphore()
    with jax.named_scope("signals"):
        for p in range(1, NY * NX):
            py, px = in_plane(p)
            pl.semaphore_signal(barrier, inc=1, device_id=(z, c, py, px), device_id_type=MESH_ID)
        for k in range(1, NSP):
            pl.semaphore_signal(barrier, inc=1, device_id=along_z(k), device_id_type=MESH_ID)

    loads = [
        pltpu.make_async_copy(far, here, load_sems.at[i])
        for i, (far, here) in enumerate(zip(away, near))
    ]
    for i in (9, 1, 2, 6, 3, 4, 0, 5, 7, 8, 10, 13, 11, 12):
        loads[i].start()

    with jax.named_scope("local"):
        for i in (1, 2, 6, 3, 0):
            loads[i].wait()
        product = ig[...].astype(F32) * ci[...].astype(F32)
        marks = doc[...].astype(F32)
        halo[0, 0:32, :] = product[:, 128:256]
        halo[0, 32:40, :] = jnp.broadcast_to(marks[:, 128:256], (8, 128))
        tap = [column_of(taps[i : i + 1, :], 32) for i in range(3)]

    with jax.named_scope("entry"):
        pl.semaphore_wait(barrier, NY * NX - 1 + NSP - 1)

    my_rows = pl.ds(pl.multiple_of(own * 32, 32), 32)

    def mix(before, before_mark, piece, mark):
        lanes = lax.broadcasted_iota(jnp.int32, (32, 128), 1)
        lane_row = lax.broadcasted_iota(jnp.int32, (1, 128), 1)
        mixed = tap[2] * piece
        for shift in (1, 2):
            back = jnp.where(
                lanes < shift, pltpu.roll(before, shift, 1), pltpu.roll(piece, shift, 1)
            )
            back_mark = jnp.where(
                lane_row < shift, pltpu.roll(before_mark, shift, 1), pltpu.roll(mark, shift, 1)
            )
            same = jnp.where(back_mark == mark, 1.0, 0.0)
            mixed = mixed + (same * tap[2 - shift]) * back
        return mixed

    def send_mixed(part):
        cols = pl.ds(part * 128, 128)
        for p in range(1, NY * NX):
            py, px = in_plane(p)
            send(co.at[my_rows, cols], co.at[my_rows, cols], "co", f"co{part}", (z, c, py, px))

    with jax.named_scope("halo_send"):
        send(halo.at[0], halo.at[1], "halo", "halo", (lax.rem(z + c, NZ), 1 - c, y, x))
        late = mix(product[:, 0:128], marks[:, 0:128], product[:, 128:256], marks[:, 128:256])
        co[my_rows, 128:256] = (og[:, 128:256].astype(F32) * late).astype(BF)
        send_mixed(1)
        loads[4].wait()
        for p in range(1, NY * NX):
            py, px = in_plane(p)
            there = py * NX + px
            send(
                ow.at[:, pl.ds(pl.multiple_of(there * 128, 128), 128)], wc.at[my_rows, :],
                "ow", "ow", (z, c, py, px),
            )
        wc[my_rows, :] = ow[:, pl.ds(pl.multiple_of(own * 128, 128), 128)]
    with jax.named_scope("halo_wait"):
        landed(halo.at[1], "halo")
    with jax.named_scope("conv"):
        first = jnp.where((z == 0) & (c == 0), 1.0, 0.0)
        prior_mark = halo[1, 32:33, :] * (1.0 - first) - first
        early = mix(halo[1, 0:32, :], prior_mark, product[:, 0:128], marks[:, 0:128])
        co[my_rows, 0:128] = (og[:, 0:128].astype(F32) * early).astype(BF)
        send_mixed(0)
    with jax.named_scope("slots"):
        for i in (5, 7, 8, 9, 10):
            loads[i].wait()
        ids = lax.broadcasted_iota(jnp.int32, (NSP, 256), 0)
        hits = [(routes[i : i + 1, :] == ids).astype(F32) for i in range(2)]
        before = (
            lax.broadcasted_iota(jnp.int32, (256, 256), 0)
            < lax.broadcasted_iota(jnp.int32, (256, 256), 1)
        ).astype(F32)
        counts = jnp.dot(
            (hits[0] + hits[1]).astype(BF), before.astype(BF), preferred_element_type=F32
        )
        slots = lax.broadcasted_iota(jnp.int32, (ROWS, 256), 0)
        for i, chosen in ((0, sp0), (1, sp1)):
            rank = jnp.sum(hits[i] * counts, axis=0, keepdims=True).astype(jnp.int32)
            expert = routes[i : i + 1, :]
            ez = jnp.right_shift(expert, 1)
            ec = expert - 2 * ez
            dz = ez - z
            dz = jnp.where(dz < 0, dz + NZ, dz)
            dc = jnp.where(ec == c, 0, 1)
            step = jnp.where(dz == 0, 0, jnp.where(dz <= NZ // 2, 2 * dz - 1, 2 * (NZ - dz)))
            place = jnp.zeros_like(step)
            for here, there in enumerate(ORDER):
                place = jnp.where(step == there, here, place)
            step = place
            slot = (step * 2 + dc) * CAP + rank
            chosen[...] = jnp.where(slots == slot, 1.0, 0.0).astype(BF)
    with jax.named_scope("residual"):
        stream_t = ALPHA * res[...].astype(F32).T

    def ring(axis, step):
        if axis == "x":
            return (z, c, y, lax.rem(x + step + NX, NX))
        return (z, c, lax.rem(y + step + NY, NY), x)

    def spot(axis, step):
        return lax.rem((x if axis == "x" else y) + step + 4, 4)

    def down_rows(half, step, part=None):
        lead = spot("yx"[half], step)
        if half == 0:
            return wdi.at[lead] if part is None else wdi.at[lead, pl.ds(2 * part, 2)]
        return wdi.at[:, lead] if part is None else wdi.at[pl.ds(2 * part, 2), lead]

    def down_cols(half, step, part=None):
        cols = pl.ds(pl.multiple_of(spot("yx"[half], step) * 128, 128), 128)
        buf = (wda, wdb)[half]
        return buf.at[:, :, cols] if part is None else buf.at[pl.ds(2 * part, 2), :, cols]

    def down_sends():
        loads[13].wait()
        for half in range(2):
            for way in range(2):
                send(
                    down_rows(half, 2, way), (wra, wrb)[half].at[way], f"down{half}",
                    f"down{half}0", ring("yx"[half], 1 - 2 * way),
                )
        for half in range(2):
            for way in range(2):
                step = 1 - 2 * way
                send(
                    down_rows(half, step), down_cols(half, 0), f"down{half}", f"down{half}1",
                    ring("yx"[half], step),
                )
        own_y = pl.ds(pl.multiple_of(y * 128, 128), 128)
        own_x = pl.ds(pl.multiple_of(x * 128, 128), 128)
        wda[:, :, own_y] = wdi[y]
        wdb[:, :, own_x] = wdi[:, x]

    def down_relay():
        for half in range(2):
            landed((wra, wrb)[half], f"down{half}0")
            for way in range(2):
                step = 1 - 2 * way
                send(
                    (wra, wrb)[half].at[way], down_cols(half, -step, way), f"down{half}",
                    f"down{half}2", ring("yx"[half], step),
                )

    def down_end():
        for half in range(2):
            buf = (wda, wdb)[half]
            landed(buf.at[:, :, pl.ds(0, 256)], f"down{half}1")
            landed(buf.at[:, :, pl.ds(0, 128)], f"down{half}2")

    with jax.named_scope("mix_wait"):
        landed(wc.at[pl.ds(0, 480), :], "ow")
        landed(co.at[pl.ds(0, 480), pl.ds(0, 128)], "co1")
        landed(co.at[pl.ds(0, 480), pl.ds(0, 128)], "co0")
    with jax.named_scope("mix_dot"):
        stream_t = stream_t + nt_dot(wc[...], co[...], ((0,), (0,)))

    def norm(stream, which, gain_col):
        s1 = jnp.sum(stream, axis=0, keepdims=True)
        s2 = jnp.sum(stream * stream, axis=0, keepdims=True)
        sub = lax.broadcasted_iota(jnp.int32, (2, 256), 0)
        st[which, own] = jnp.where(sub == 0, s1, s2)
        for p in range(1, NY * NX):
            py, px = in_plane(p)
            send(st.at[which, own], st.at[which, own], f"st{which}", f"st{which}", (z, c, py, px))
        if which == 0:
            down_sends()
        landed(st.at[which, pl.ds(0, 15)], f"st{which}")
        total = st[which, 0]
        for j in range(1, NY * NX):
            total = total + st[which, j]
        mean = total[0:1, :] / D
        spread = total[1:2, :] / D - mean * mean
        return (stream - mean) * lax.rsqrt(spread + EPSILON) * gain_col

    with jax.named_scope("norm_a"):
        normed_t = norm(stream_t, 0, column_of(mg[...], 128)).astype(BF)
    nrm[...] = normed_t

    def rows_of(g):
        return pl.ds(STARTS[g] * 64, SIZES[g] * 64)

    def ks_of(g):
        return range(STARTS[g] * 2, (STARTS[g] + SIZES[g]) * 2)

    with jax.named_scope("dispatch"):
        for g in range(GROUPS):
            rows = rows_of(g)
            chosen = sp0[rows, :] + sp1[rows, :]
            sb[rows, :] = nt_dot(chosen, normed_t, ((1,), (1,))).astype(BF)
            for k in ks_of(g):
                cut = pl.ds(k * CAP, CAP)
                if k == 0:
                    x4[y, x, cut, :] = sb[cut, :]
                else:
                    send(sb.at[cut, :], x4.at[y, x, cut, :], "z", f"z{g}", along_z(k))
    with jax.named_scope("down_relay"):
        down_relay()

    def span(g, half, part):
        length = SIZES[g] * 32
        start = STARTS[g] * 64 + half * length
        if part == "lo":
            return pl.ds(start, length // 2)
        if part == "hi":
            return pl.ds(start + length // 2, length // 2)
        return pl.ds(start, length)

    def slab(buf, g, half, phase, step, part=None):
        rows = span(g, half, part)
        if half == 0:
            if phase == 0:
                return buf.at[y, spot("x", step), rows, :]
            return buf.at[spot("y", step), :, rows, :]
        if phase == 0:
            return buf.at[spot("y", step), x, rows, :]
        return buf.at[:, spot("x", step), rows, :]

    def axis_of(half, phase):
        return "xy"[(half + phase) % 2]

    def steps_of(g, chosen):
        return (1, -1, 2) if g in chosen else (1, -1)

    def ag_like(g, phase, count):
        if phase == 0:
            return x4.at[0, pl.ds(0, count), rows_of(g), :]
        return x4.at[pl.ds(0, count), :, rows_of(g), :]

    def ag_send(g):
        for half in range(2):
            for step in steps_of(g, GATHER_DIRECT):
                mine = slab(x4, g, half, 0, 0)
                send(mine, mine, f"x0{g}", f"x0d{g}", ring(axis_of(half, 0), step))

    def ag_onward(g, places):
        for place in places:
            for half in range(2):
                for step in steps_of(g, GATHER_DIRECT):
                    piece = slab(x4, g, half, 0, place)
                    send(piece, piece, f"x1{g}", f"x1d{g}", ring(axis_of(half, 1), step))

    def ag_relay(g, phase):
        landed(ag_like(g, phase, 2), f"x{phase}d{g}")
        for half in range(2):
            for step, part in ((1, "lo"), (-1, "hi")):
                piece = slab(x4, g, half, phase, -step, part)
                send(
                    piece, piece, f"x{phase}{g}", f"x{phase}r{g}", ring(axis_of(half, phase), step)
                )

    def ag_end(g, phase):
        if g in GATHER_DIRECT:
            landed(ag_like(g, phase, 3), f"x{phase}d{g}")
        else:
            landed(ag_like(g, phase, 1), f"x{phase}r{g}")

    def expert_in(g):
        rows = rows_of(g)
        inputs = jnp.concatenate(
            [x4[b, a, rows, :] for b in range(NY) for a in range(NX)], axis=1
        )
        gate = jnp.minimum(jnp.dot(inputs, wg[...], preferred_element_type=F32), LIMIT)
        up = jnp.clip(jnp.dot(inputs, wu[...], preferred_element_type=F32), -LIMIT, LIMIT)
        hidden = ((up + 1.0) * gate * jax.nn.sigmoid(SLOPE * gate)).astype(BF)
        for half in range(2):
            h4[spot("xy"[half], 0), span(g, half, None), :] = hidden[
                half * SIZES[g] * 32 : (half + 1) * SIZES[g] * 32, :
            ]

    def hidden_at(g, half, step, part=None):
        return h4.at[spot("xy"[half], step), span(g, half, part), :]

    def hidden_send(g):
        for half in range(2):
            for step in steps_of(g, SUM_DIRECT):
                mine = hidden_at(g, half, 0)
                send(mine, mine, f"h{g}", f"hd{g}", ring("xy"[half], step))

    def hidden_relay(g):
        landed(h4.at[pl.ds(0, 2), rows_of(g), :], f"hd{g}")
        for half in range(2):
            for step, part in ((1, "lo"), (-1, "hi")):
                piece = hidden_at(g, half, -step, part)
                send(piece, piece, f"h{g}", f"hr{g}", ring("xy"[half], step))

    def hidden_end(g):
        if g in SUM_DIRECT:
            landed(h4.at[pl.ds(0, 3), rows_of(g), :], f"hd{g}")
        else:
            landed(h4.at[pl.ds(0, 1), rows_of(g), :], f"hr{g}")

    def expert_out(g):
        for half in range(2):
            rows = span(g, half, None)
            inputs = jnp.concatenate([h4[b, rows, :] for b in range(4)], axis=1)
            weights = (wda, wdb)[half][...].reshape(1024, 512)
            part = jnp.dot(inputs, weights, preferred_element_type=F32).astype(BF)
            for b in range(4):
                p4[b, rows, :] = part[:, b * 128 : (b + 1) * 128]

    def part_at(g, half, step, part=None):
        return p4.at[spot("yx"[half], step), span(g, half, part), :]

    def first_at(g, half, way):
        return r1.at[half, way, pl.ds(STARTS[g] * 16, SIZES[g] * 16), :]

    def second_at(g, half, way):
        return r2.at[half, way, pl.ds(STARTS[g] * 32, SIZES[g] * 32), :]

    def sum_first(g):
        for half in range(2):
            axis = "yx"[half]
            if g in SUM_DIRECT:
                for way, step in enumerate(steps_of(g, SUM_DIRECT)):
                    send(
                        part_at(g, half, step), second_at(g, half, way), f"s{g}", f"sd{g}",
                        ring(axis, step),
                    )
            else:
                for way, part in ((0, "lo"), (1, "hi")):
                    send(
                        part_at(g, half, 2, part), first_at(g, half, way), f"s{g}", f"sr{g}",
                        ring(axis, 1 - 2 * way),
                    )

    def sum_second(g):
        landed(p4.at[pl.ds(0, 1), rows_of(g), :], f"sr{g}")
        for half in range(2):
            for way, part in ((0, "lo"), (1, "hi")):
                step = 1 - 2 * way
                edge = part_at(g, half, step, part)
                came = first_at(g, half, way)
                edge[...] = (edge[...].astype(F32) + came[...].astype(F32)).astype(BF)
                send(
                    part_at(g, half, step), second_at(g, half, way), f"s{g}", f"sd{g}",
                    ring("yx"[half], step),
                )

    def sum_end(g):
        ways = len(steps_of(g, SUM_DIRECT))
        landed(p4.at[pl.ds(0, ways), rows_of(g), :], f"sd{g}")
        for half in range(2):
            total = part_at(g, half, 0)[...].astype(F32)
            for way in range(ways):
                total = total + second_at(g, half, way)[...].astype(F32)
            ob[span(g, half, None), :] = total.astype(BF)

    first_of = {stage: g for stage, g in reversed(SCHEDULE)}
    for stage, g in SCHEDULE:
        with jax.named_scope(f"{stage}_{g}"):
            if stage == "a0":
                skip = CAP if g == 0 else 0
                arrived = pl.ds(STARTS[g] * 64 + skip, SIZES[g] * 64 - skip)
                landed(x4.at[y, x, arrived, :], f"z{g}")
                ag_send(g)
                ag_onward(g, (0,))
            elif stage == "a1":
                ag_relay(g, 0)
                ag_onward(g, (-1, 1))
            elif stage == "a2":
                ag_end(g, 0)
                ag_onward(g, (-1, 1, 2) if g in GATHER_DIRECT else (2,))
            elif stage == "a3":
                ag_relay(g, 1)
            elif stage == "c":
                ag_end(g, 1)
                if g == first_of["c"]:
                    loads[11].wait()
                    loads[12].wait()
                expert_in(g)
                hidden_send(g)
            elif stage == "h1":
                hidden_relay(g)
            elif stage == "d":
                hidden_end(g)
                if g == first_of["d"]:
                    down_end()
                expert_out(g)
                sum_first(g)
            elif stage == "e1":
                sum_second(g)
            else:
                sum_end(g)
                for k in ks_of(g):
                    cut = pl.ds(k * CAP, CAP)
                    if k == 0:
                        ret[cut, :] = ob[cut, :]
                    else:
                        send(ob.at[cut, :], ret.at[cut, :], "ret", "ret", back_z(k))

    with jax.named_scope("drain"):
        drained(halo.at[0], "halo")
        drained(wc.at[pl.ds(0, 480), :], "ow")
        drained(co.at[pl.ds(0, 480), :], "co")
        drained(st.at[0, pl.ds(0, 15)], "st0")
        drained(wda, "down0")
        drained(wdb, "down1")
        drained(sb.at[pl.ds(CAP, ROWS - CAP), :], "z")
        for g in range(GROUPS):
            drained(ag_like(g, 0, 3), f"x0{g}")
            drained(ag_like(g, 1, 3), f"x1{g}")
            drained(h4.at[pl.ds(0, 3), rows_of(g), :], f"h{g}")
            drained(p4.at[pl.ds(0, 3), rows_of(g), :], f"s{g}")
    with jax.named_scope("ret_wait"):
        landed(ret.at[pl.ds(CAP, ROWS - CAP), :], "ret")
    with jax.named_scope("combine"):
        results = ret[...]
        ffn = rw[0:1, :] * nt_dot(results, sp0[...], ((0,), (0,)))
        ffn = ffn + rw[1:2, :] * nt_dot(results, sp1[...], ((0,), (0,)))
        second = ALPHA * nrm[...].astype(F32) + ffn
    with jax.named_scope("norm_b"):
        out[...] = norm(second, 1, column_of(fg[...], 128)).T.astype(BF)
    drained(st.at[1, pl.ds(0, 15)], "st1")
    drained(ob.at[pl.ds(CAP, ROWS - CAP), :], "ret")


def per_device(
    out_gate, in_gate, conv_input, conv_taps, out_weight, residual, document, mix_gain,
    ffn_gain, routes, route_weight, expert_gate, expert_up, expert_down,
):
    args = (
        out_gate.T, in_gate.T, conv_input.T, conv_taps, out_weight, residual,
        document[None, :], mix_gain[None, :], ffn_gain[None, :], routes.T, route_weight.T,
        expert_gate[0], expert_up[0], expert_down[0].reshape(NY, NX, 256, 128),
    )
    args = tuple(pltpu.with_memory_space_constraint(arg, pltpu.HBM) for arg in args)
    dma = pltpu.SemaphoreType.DMA
    scratch = [pltpu.VMEM(arg.shape, arg.dtype) for arg in args] + [
        pltpu.VMEM((2, 40, 128), F32),
        pltpu.VMEM((512, 256), BF),
        pltpu.VMEM((512, 128), BF),
        pltpu.VMEM((4, 256, 512), BF),
        pltpu.VMEM((4, 256, 512), BF),
        pltpu.VMEM((2, 2, 256, 128), BF),
        pltpu.VMEM((2, 2, 256, 128), BF),
        pltpu.VMEM((2, 16, 2, 256), F32),
        pltpu.VMEM((ROWS, 256), BF),
        pltpu.VMEM((ROWS, 256), BF),
        pltpu.VMEM((ROWS, 128), BF),
        pltpu.VMEM((NY, NX, ROWS, 128), BF),
        pltpu.VMEM((4, ROWS, 256), BF),
        pltpu.VMEM((4, ROWS, 128), BF),
        pltpu.VMEM((2, 2, ROWS // 4, 128), BF),
        pltpu.VMEM((2, 3, ROWS // 2, 128), BF),
        pltpu.VMEM((ROWS, 128), BF),
        pltpu.VMEM((ROWS, 128), BF),
        pltpu.VMEM((128, 256), BF),
        dma((len(args),)),
        dma((len(SENT),)),
        dma((len(RECV),)),
    ]
    return pl.pallas_call(
        kernel,
        out_shape=jax.ShapeDtypeStruct((256, 128), BF),
        in_specs=[pl.BlockSpec(memory_space=pl.ANY)] * len(args),
        out_specs=pl.BlockSpec(memory_space=pltpu.VMEM),
        scratch_shapes=scratch,
        compiler_params=pltpu.CompilerParams(
            collective_id=0, has_side_effects=True, vmem_limit_bytes=48 * 1024 * 1024
        ),
    )(*args)


def solution(mesh):
    torus = Mesh(mesh.devices.reshape(NZ, NC, NY, NX), ("z", "c", "y", "x"))
    sp, tp = ("z", "c"), ("y", "x")
    in_specs = (
        P(sp, tp), P(sp, tp), P(sp, tp), P(None, tp), P(tp, None), P(sp, tp), P(sp), P(tp),
        P(tp), P(sp, None), P(sp, None), P(sp, None, tp), P(sp, None, tp), P(sp, None, tp),
    )
    return jax.shard_map(
        per_device, mesh=torus, in_specs=in_specs, out_specs=P(sp, tp), check_vma=False
    )
```

```python
import jax
import jax.numpy as jnp
from jax import lax
from jax.experimental import pallas as pl
from jax.experimental.pallas import tpu as pltpu
from jax.sharding import Mesh
from jax.sharding import PartitionSpec as P

D = 2048
CAP = 32
ALPHA = 8.0**0.25
EPSILON = 1e-05
LIMIT = 7.0
SLOPE = 1.702
MESH_ID = pl.DeviceIdType.MESH
BF = jnp.bfloat16
F32 = jnp.float32

NZ, NC, NY, NX = 16, 2, 4, 4
NSP = NZ * NC
ROWS = NSP * CAP
SIZES = (1, 2, 4, 4, 2, 2, 1)
GROUPS = len(SIZES)
STARTS = tuple(sum(SIZES[:g]) for g in range(GROUPS))
ORDER = tuple(range(16))
GATHER_DIRECT = (0,)
SUM_DIRECT = (5, 6)


def z_shift(k):
    step, side = k // 2, k % 2
    step = ORDER[step]
    if step == 0:
        return 0, side
    return ((step + 1) // 2 if step % 2 else NZ - step // 2), side


SCHEDULE = [
    ("a0", 1), ("a0", 0), ("a0", 2), ("a1", 1), ("a2", 0), ("a1", 2), ("a0", 4), ("a0", 3),
    ("a2", 2), ("a0", 5), ("a1", 4), ("a1", 3), ("a0", 6), ("a1", 5), ("a2", 4), ("a2", 3),
    ("a2", 1), ("a1", 6), ("a2", 5), ("a3", 2), ("a3", 4), ("c", 0), ("a2", 6), ("a3", 5),
    ("a3", 3), ("a3", 1), ("a3", 6), ("c", 4), ("c", 5), ("c", 3), ("h1", 4), ("c", 6), ("c", 2),
    ("h1", 3), ("d", 5), ("c", 1), ("d", 4), ("h1", 2), ("d", 6), ("h1", 0), ("d", 3), ("h1", 1),
    ("e2", 5), ("e1", 4), ("d", 2), ("d", 0), ("e2", 6), ("e1", 3), ("d", 1), ("e2", 4),
    ("e1", 2), ("e2", 3), ("e1", 0), ("e1", 1), ("e2", 2), ("e2", 0), ("e2", 1),
]


PEERS = sorted(
    range(1, NY * NX), key=lambda p: -min(p // NX, NY - p // NX) - min(p % NX, NX - p % NX)
)
NAMES = (
    ["halo", "ow", "co0", "co1", "st0", "st1", "ret"]
    + [f"down{h}{n}" for h in range(2) for n in range(3)]
    + [f"z{g}" for g in range(GROUPS)]
    + [f"{n}{g}" for g in range(GROUPS) for n in ("x0d", "x0r", "x1d", "x1r", "hd", "hr", "sd", "sr")]
)
RECV = {name: i for i, name in enumerate(NAMES)}
SENT_NAMES = ("halo", "ow", "co", "st0", "st1", "ret", "down0", "down1", "z", "x", "h", "s")
SENT = {name: i for i, name in enumerate(SENT_NAMES)}


def column_of(row_ref, size):
    eye = lax.broadcasted_iota(jnp.int32, (size, size), 0) == lax.broadcasted_iota(
        jnp.int32, (size, size), 1
    )
    row = jnp.broadcast_to(row_ref, (size, size))
    return jnp.sum(jnp.where(eye, row, 0.0), axis=1, keepdims=True)


def nt_dot(a, b, dims):
    return lax.dot_general(a, b, (dims, ((), ())), preferred_element_type=F32)


def kernel(*refs):
    away, out, near = refs[:14], refs[14], refs[15:29]
    og, ig, ci, taps, ow, res, doc, mg, fg, routes, rw, wg, wu, wdi = near
    (
        halo, co, wc, wda, wdb, wra, wrb, st, sp0, sp1, sb, x4, h4, p4, r1, r2, ob, ret, nrm,
        load_sems, sent_sems, recv_sems,
    ) = refs[29:]
    z, c = lax.axis_index("z"), lax.axis_index("c")
    y, x = lax.axis_index("y"), lax.axis_index("x")
    own = y * NX + x

    def send(src, dst, sent, recv, target):
        pltpu.make_async_remote_copy(
            src_ref=src,
            dst_ref=dst,
            send_sem=sent_sems.at[SENT[sent]],
            recv_sem=recv_sems.at[RECV[recv]],
            device_id=target,
            device_id_type=MESH_ID,
        ).start()

    def landed(like, recv):
        pltpu.make_async_remote_copy(
            src_ref=like,
            dst_ref=like,
            send_sem=sent_sems.at[0],
            recv_sem=recv_sems.at[RECV[recv]],
            device_id=(z, c, y, lax.rem(x + 1, NX)),
            device_id_type=MESH_ID,
        ).wait_recv()

    def drained(like, sent):
        pltpu.make_async_remote_copy(
            src_ref=like,
            dst_ref=like,
            send_sem=sent_sems.at[SENT[sent]],
            recv_sem=recv_sems.at[0],
            device_id=(z, c, y, lax.rem(x + 1, NX)),
            device_id_type=MESH_ID,
        ).wait_send()

    def in_plane(p):
        return lax.rem(y + p // NX, NY), lax.rem(x + p % NX, NX)

    def from_plane(p):
        return lax.rem(y + NY - p // NX, NY), lax.rem(x + NX - p % NX, NX)

    def along_z(k):
        dz, dc = z_shift(k)
        return (lax.rem(z + dz, NZ), lax.rem(c + dc, NC), y, x)

    def back_z(k):
        dz, dc = z_shift(k)
        return (lax.rem(z + NZ - dz, NZ), lax.rem(c + NC - dc, NC), y, x)

    barrier = pltpu.get_barrier_semaphore()
    loads = [
        pltpu.make_async_copy(far, here, load_sems.at[i])
        for i, (far, here) in enumerate(zip(away, near))
    ]
    for i in (1, 2, 6, 3, 0):
        loads[i].start()
    with jax.named_scope("signals"):
        for p in PEERS:
            py, px = in_plane(p)
            pl.semaphore_signal(barrier, inc=1, device_id=(z, c, py, px), device_id_type=MESH_ID)
        for k in range(1, NSP):
            pl.semaphore_signal(barrier, inc=1, device_id=along_z(k), device_id_type=MESH_ID)

    for i in (4, 9, 5, 7, 8, 10, 13, 11, 12):
        loads[i].start()

    with jax.named_scope("local"):
        for i in (1, 2, 6, 3, 0):
            loads[i].wait()
        product = ig[...].astype(F32) * ci[...].astype(F32)
        marks = doc[...].astype(F32)
        halo[0, 0:32, :] = product[:, 128:256]
        halo[0, 32:40, :] = jnp.broadcast_to(marks[:, 128:256], (8, 128))
        tap = [column_of(taps[i : i + 1, :], 32) for i in range(3)]

    with jax.named_scope("entry"):
        pl.semaphore_wait(barrier, NY * NX - 1 + NSP - 1)

    my_rows = pl.ds(pl.multiple_of(own * 32, 32), 32)

    def mix(before, before_mark, piece, mark):
        lanes = lax.broadcasted_iota(jnp.int32, (32, 128), 1)
        lane_row = lax.broadcasted_iota(jnp.int32, (1, 128), 1)
        mixed = tap[2] * piece
        for shift in (1, 2):
            back = jnp.where(
                lanes < shift, pltpu.roll(before, shift, 1), pltpu.roll(piece, shift, 1)
            )
            back_mark = jnp.where(
                lane_row < shift, pltpu.roll(before_mark, shift, 1), pltpu.roll(mark, shift, 1)
            )
            same = jnp.where(back_mark == mark, 1.0, 0.0)
            mixed = mixed + (same * tap[2 - shift]) * back
        return mixed

    def send_mixed(part):
        cols = pl.ds(part * 128, 128)
        for p in PEERS:
            py, px = in_plane(p)
            send(co.at[my_rows, cols], co.at[my_rows, cols], "co", f"co{part}", (z, c, py, px))

    with jax.named_scope("halo_send"):
        send(halo.at[0], halo.at[1], "halo", "halo", (lax.rem(z + c, NZ), 1 - c, y, x))
        late = mix(product[:, 0:128], marks[:, 0:128], product[:, 128:256], marks[:, 128:256])
        co[my_rows, 128:256] = (og[:, 128:256].astype(F32) * late).astype(BF)
        send_mixed(1)
        loads[4].wait()
        for p in PEERS:
            py, px = in_plane(p)
            there = py * NX + px
            send(
                ow.at[:, pl.ds(pl.multiple_of(there * 128, 128), 128)], wc.at[my_rows, :],
                "ow", "ow", (z, c, py, px),
            )
        wc[my_rows, :] = ow[:, pl.ds(pl.multiple_of(own * 128, 128), 128)]
    with jax.named_scope("halo_wait"):
        landed(halo.at[1], "halo")
    with jax.named_scope("conv"):
        first = jnp.where((z == 0) & (c == 0), 1.0, 0.0)
        prior_mark = halo[1, 32:33, :] * (1.0 - first) - first
        early = mix(halo[1, 0:32, :], prior_mark, product[:, 0:128], marks[:, 0:128])
        co[my_rows, 0:128] = (og[:, 0:128].astype(F32) * early).astype(BF)
        send_mixed(0)
    with jax.named_scope("slots"):
        for i in (5, 7, 8, 9, 10):
            loads[i].wait()
        ids = lax.broadcasted_iota(jnp.int32, (NSP, 256), 0)
        hits = [(routes[i : i + 1, :] == ids).astype(F32) for i in range(2)]
        before = (
            lax.broadcasted_iota(jnp.int32, (256, 256), 0)
            < lax.broadcasted_iota(jnp.int32, (256, 256), 1)
        ).astype(F32)
        counts = jnp.dot(
            (hits[0] + hits[1]).astype(BF), before.astype(BF), preferred_element_type=F32
        )
        slots = lax.broadcasted_iota(jnp.int32, (ROWS, 256), 0)
        for i, chosen in ((0, sp0), (1, sp1)):
            rank = jnp.sum(hits[i] * counts, axis=0, keepdims=True).astype(jnp.int32)
            expert = routes[i : i + 1, :]
            ez = jnp.right_shift(expert, 1)
            ec = expert - 2 * ez
            dz = ez - z
            dz = jnp.where(dz < 0, dz + NZ, dz)
            dc = jnp.where(ec == c, 0, 1)
            step = jnp.where(dz == 0, 0, jnp.where(dz <= NZ // 2, 2 * dz - 1, 2 * (NZ - dz)))
            place = jnp.zeros_like(step)
            for here, there in enumerate(ORDER):
                place = jnp.where(step == there, here, place)
            step = place
            slot = (step * 2 + dc) * CAP + rank
            chosen[...] = jnp.where(slots == slot, 1.0, 0.0).astype(BF)
    with jax.named_scope("residual"):
        stream_t = ALPHA * res[...].astype(F32).T

    def ring(axis, step):
        if axis == "x":
            return (z, c, y, lax.rem(x + step + NX, NX))
        return (z, c, lax.rem(y + step + NY, NY), x)

    def spot(axis, step):
        return lax.rem((x if axis == "x" else y) + step + 4, 4)

    def down_rows(half, step, part=None):
        lead = spot("yx"[half], step)
        if half == 0:
            return wdi.at[lead] if part is None else wdi.at[lead, pl.ds(2 * part, 2)]
        return wdi.at[:, lead] if part is None else wdi.at[pl.ds(2 * part, 2), lead]

    def down_cols(half, step, part=None):
        cols = pl.ds(pl.multiple_of(spot("yx"[half], step) * 128, 128), 128)
        buf = (wda, wdb)[half]
        return buf.at[:, :, cols] if part is None else buf.at[pl.ds(2 * part, 2), :, cols]

    def down_sends():
        loads[13].wait()
        for half in range(2):
            for way in range(2):
                send(
                    down_rows(half, 2, way), (wra, wrb)[half].at[way], f"down{half}",
                    f"down{half}0", ring("yx"[half], 1 - 2 * way),
                )
        for half in range(2):
            for way in range(2):
                step = 1 - 2 * way
                send(
                    down_rows(half, step), down_cols(half, 0), f"down{half}", f"down{half}1",
                    ring("yx"[half], step),
                )
        own_y = pl.ds(pl.multiple_of(y * 128, 128), 128)
        own_x = pl.ds(pl.multiple_of(x * 128, 128), 128)
        wda[:, :, own_y] = wdi[y]
        wdb[:, :, own_x] = wdi[:, x]

    def down_relay():
        for half in range(2):
            landed((wra, wrb)[half], f"down{half}0")
            for way in range(2):
                step = 1 - 2 * way
                send(
                    (wra, wrb)[half].at[way], down_cols(half, -step, way), f"down{half}",
                    f"down{half}2", ring("yx"[half], step),
                )

    def down_end():
        for half in range(2):
            buf = (wda, wdb)[half]
            landed(buf.at[:, :, pl.ds(0, 256)], f"down{half}1")
            landed(buf.at[:, :, pl.ds(0, 128)], f"down{half}2")

    with jax.named_scope("mix_wait"):
        landed(wc.at[pl.ds(0, 480), :], "ow")
        landed(co.at[pl.ds(0, 480), pl.ds(0, 128)], "co1")
        landed(co.at[pl.ds(0, 480), pl.ds(0, 128)], "co0")
    with jax.named_scope("mix_dot"):
        stream_t = stream_t + nt_dot(wc[...], co[...], ((0,), (0,)))

    def norm(stream, which, gain_col):
        s1 = jnp.sum(stream, axis=0, keepdims=True)
        s2 = jnp.sum(stream * stream, axis=0, keepdims=True)
        sub = lax.broadcasted_iota(jnp.int32, (2, 256), 0)
        st[which, own] = jnp.where(sub == 0, s1, s2)
        for p in PEERS:
            py, px = in_plane(p)
            send(st.at[which, own], st.at[which, own], f"st{which}", f"st{which}", (z, c, py, px))
        if which == 0:
            down_sends()
        landed(st.at[which, pl.ds(0, 15)], f"st{which}")
        total = st[which, 0]
        for j in range(1, NY * NX):
            total = total + st[which, j]
        mean = total[0:1, :] / D
        spread = total[1:2, :] / D - mean * mean
        return (stream - mean) * lax.rsqrt(spread + EPSILON) * gain_col

    with jax.named_scope("norm_a"):
        normed_t = norm(stream_t, 0, column_of(mg[...], 128)).astype(BF)
    nrm[...] = normed_t

    def rows_of(g):
        return pl.ds(STARTS[g] * 64, SIZES[g] * 64)

    def ks_of(g):
        return range(STARTS[g] * 2, (STARTS[g] + SIZES[g]) * 2)

    with jax.named_scope("dispatch"):
        for g in range(GROUPS):
            rows = rows_of(g)
            chosen = sp0[rows, :] + sp1[rows, :]
            sb[rows, :] = nt_dot(chosen, normed_t, ((1,), (1,))).astype(BF)
            for k in ks_of(g):
                cut = pl.ds(k * CAP, CAP)
                if k == 0:
                    x4[y, x, cut, :] = sb[cut, :]
                else:
                    send(sb.at[cut, :], x4.at[y, x, cut, :], "z", f"z{g}", along_z(k))
    with jax.named_scope("down_relay"):
        down_relay()

    def span(g, half, part):
        length = SIZES[g] * 32
        start = STARTS[g] * 64 + half * length
        if part == "lo":
            return pl.ds(start, length // 2)
        if part == "hi":
            return pl.ds(start + length // 2, length // 2)
        return pl.ds(start, length)

    def slab(buf, g, half, phase, step, part=None):
        rows = span(g, half, part)
        if half == 0:
            if phase == 0:
                return buf.at[y, spot("x", step), rows, :]
            return buf.at[spot("y", step), :, rows, :]
        if phase == 0:
            return buf.at[spot("y", step), x, rows, :]
        return buf.at[:, spot("x", step), rows, :]

    def axis_of(half, phase):
        return "xy"[(half + phase) % 2]

    def steps_of(g, chosen):
        return (1, -1, 2) if g in chosen else (1, -1)

    def ag_like(g, phase, count):
        if phase == 0:
            return x4.at[0, pl.ds(0, count), rows_of(g), :]
        return x4.at[pl.ds(0, count), :, rows_of(g), :]

    def ag_send(g):
        for half in range(2):
            for step in steps_of(g, GATHER_DIRECT):
                mine = slab(x4, g, half, 0, 0)
                send(mine, mine, "x", f"x0d{g}", ring(axis_of(half, 0), step))

    def ag_onward(g, places):
        for place in places:
            for half in range(2):
                for step in steps_of(g, GATHER_DIRECT):
                    piece = slab(x4, g, half, 0, place)
                    send(piece, piece, "x", f"x1d{g}", ring(axis_of(half, 1), step))

    def ag_relay(g, phase):
        landed(ag_like(g, phase, 2), f"x{phase}d{g}")
        for half in range(2):
            for step, part in ((1, "lo"), (-1, "hi")):
                piece = slab(x4, g, half, phase, -step, part)
                send(
                    piece, piece, "x", f"x{phase}r{g}", ring(axis_of(half, phase), step)
                )

    def ag_end(g, phase):
        if g in GATHER_DIRECT:
            landed(ag_like(g, phase, 3), f"x{phase}d{g}")
        else:
            landed(ag_like(g, phase, 1), f"x{phase}r{g}")

    def expert_in(g):
        rows = rows_of(g)
        inputs = jnp.concatenate(
            [x4[b, a, rows, :] for b in range(NY) for a in range(NX)], axis=1
        )
        gate = jnp.minimum(jnp.dot(inputs, wg[...], preferred_element_type=F32), LIMIT)
        up = jnp.clip(jnp.dot(inputs, wu[...], preferred_element_type=F32), -LIMIT, LIMIT)
        hidden = ((up + 1.0) * gate * jax.nn.sigmoid(SLOPE * gate)).astype(BF)
        for half in range(2):
            h4[spot("xy"[half], 0), span(g, half, None), :] = hidden[
                half * SIZES[g] * 32 : (half + 1) * SIZES[g] * 32, :
            ]

    def hidden_at(g, half, step, part=None):
        return h4.at[spot("xy"[half], step), span(g, half, part), :]

    def hidden_send(g):
        for half in range(2):
            for step in steps_of(g, SUM_DIRECT):
                mine = hidden_at(g, half, 0)
                send(mine, mine, "h", f"hd{g}", ring("xy"[half], step))

    def hidden_relay(g):
        landed(h4.at[pl.ds(0, 2), rows_of(g), :], f"hd{g}")
        for half in range(2):
            for step, part in ((1, "lo"), (-1, "hi")):
                piece = hidden_at(g, half, -step, part)
                send(piece, piece, "h", f"hr{g}", ring("xy"[half], step))

    def hidden_end(g):
        if g in SUM_DIRECT:
            landed(h4.at[pl.ds(0, 3), rows_of(g), :], f"hd{g}")
        else:
            landed(h4.at[pl.ds(0, 1), rows_of(g), :], f"hr{g}")

    def expert_out(g):
        for half in range(2):
            rows = span(g, half, None)
            inputs = jnp.concatenate([h4[b, rows, :] for b in range(4)], axis=1)
            weights = (wda, wdb)[half][...].reshape(1024, 512)
            part = jnp.dot(inputs, weights, preferred_element_type=F32).astype(BF)
            for b in range(4):
                p4[b, rows, :] = part[:, b * 128 : (b + 1) * 128]

    def part_at(g, half, step, part=None):
        return p4.at[spot("yx"[half], step), span(g, half, part), :]

    def first_at(g, half, way):
        return r1.at[half, way, pl.ds(STARTS[g] * 16, SIZES[g] * 16), :]

    def second_at(g, half, way):
        return r2.at[half, way, pl.ds(STARTS[g] * 32, SIZES[g] * 32), :]

    def sum_first(g):
        for half in range(2):
            axis = "yx"[half]
            if g in SUM_DIRECT:
                for way, step in enumerate(steps_of(g, SUM_DIRECT)):
                    send(
                        part_at(g, half, step), second_at(g, half, way), "s", f"sd{g}",
                        ring(axis, step),
                    )
            else:
                for way, part in ((0, "lo"), (1, "hi")):
                    send(
                        part_at(g, half, 2, part), first_at(g, half, way), "s", f"sr{g}",
                        ring(axis, 1 - 2 * way),
                    )

    def sum_second(g):
        landed(p4.at[pl.ds(0, 1), rows_of(g), :], f"sr{g}")
        for half in range(2):
            for way, part in ((0, "lo"), (1, "hi")):
                step = 1 - 2 * way
                edge = part_at(g, half, step, part)
                came = first_at(g, half, way)
                edge[...] = (edge[...].astype(F32) + came[...].astype(F32)).astype(BF)
                send(
                    part_at(g, half, step), second_at(g, half, way), "s", f"sd{g}",
                    ring("yx"[half], step),
                )

    def sum_end(g):
        ways = len(steps_of(g, SUM_DIRECT))
        landed(p4.at[pl.ds(0, ways), rows_of(g), :], f"sd{g}")
        for half in range(2):
            total = part_at(g, half, 0)[...].astype(F32)
            for way in range(ways):
                total = total + second_at(g, half, way)[...].astype(F32)
            ob[span(g, half, None), :] = total.astype(BF)

    first_of = {stage: g for stage, g in reversed(SCHEDULE)}
    for stage, g in SCHEDULE:
        with jax.named_scope(f"{stage}_{g}"):
            if stage == "a0":
                skip = CAP if g == 0 else 0
                arrived = pl.ds(STARTS[g] * 64 + skip, SIZES[g] * 64 - skip)
                landed(x4.at[y, x, arrived, :], f"z{g}")
                ag_send(g)
                ag_onward(g, (0,))
            elif stage == "a1":
                ag_relay(g, 0)
                ag_onward(g, (-1, 1))
            elif stage == "a2":
                ag_end(g, 0)
                ag_onward(g, (-1, 1, 2) if g in GATHER_DIRECT else (2,))
            elif stage == "a3":
                ag_relay(g, 1)
            elif stage == "c":
                ag_end(g, 1)
                if g == first_of["c"]:
                    loads[11].wait()
                    loads[12].wait()
                expert_in(g)
                hidden_send(g)
            elif stage == "h1":
                hidden_relay(g)
            elif stage == "d":
                hidden_end(g)
                if g == first_of["d"]:
                    down_end()
                expert_out(g)
                sum_first(g)
            elif stage == "e1":
                sum_second(g)
            else:
                sum_end(g)
                for k in ks_of(g):
                    cut = pl.ds(k * CAP, CAP)
                    if k == 0:
                        ret[cut, :] = ob[cut, :]
                    else:
                        send(ob.at[cut, :], ret.at[cut, :], "ret", "ret", back_z(k))

    with jax.named_scope("drain"):
        drained(halo.at[0], "halo")
        drained(wc.at[pl.ds(0, 480), :], "ow")
        drained(co.at[pl.ds(0, 480), :], "co")
        drained(st.at[0, pl.ds(0, 15)], "st0")
        drained(wda, "down0")
        drained(wdb, "down1")
        drained(sb.at[pl.ds(CAP, ROWS - CAP), :], "z")
        drained(x4.at[:, :, pl.ds(0, ROWS // 16 * 15), :], "x")
        drained(h4.at[pl.ds(0, 3)], "h")
        drained(p4.at[pl.ds(0, 3)], "s")
    with jax.named_scope("ret_wait"):
        landed(ret.at[pl.ds(CAP, ROWS - CAP), :], "ret")
    with jax.named_scope("combine"):
        results = ret[...]
        ffn = rw[0:1, :] * nt_dot(results, sp0[...], ((0,), (0,)))
        ffn = ffn + rw[1:2, :] * nt_dot(results, sp1[...], ((0,), (0,)))
        second = ALPHA * nrm[...].astype(F32) + ffn
    with jax.named_scope("norm_b"):
        out[...] = norm(second, 1, column_of(fg[...], 128)).T.astype(BF)
    drained(st.at[1, pl.ds(0, 15)], "st1")
    drained(ob.at[pl.ds(CAP, ROWS - CAP), :], "ret")


def per_device(
    out_gate, in_gate, conv_input, conv_taps, out_weight, residual, document, mix_gain,
    ffn_gain, routes, route_weight, expert_gate, expert_up, expert_down,
):
    args = (
        out_gate.T, in_gate.T, conv_input.T, conv_taps, out_weight, residual,
        document[None, :], mix_gain[None, :], ffn_gain[None, :], routes.T, route_weight.T,
        expert_gate[0], expert_up[0], expert_down[0].reshape(NY, NX, 256, 128),
    )
    args = tuple(pltpu.with_memory_space_constraint(arg, pltpu.HBM) for arg in args)
    dma = pltpu.SemaphoreType.DMA
    scratch = [pltpu.VMEM(arg.shape, arg.dtype) for arg in args] + [
        pltpu.VMEM((2, 40, 128), F32),
        pltpu.VMEM((512, 256), BF),
        pltpu.VMEM((512, 128), BF),
        pltpu.VMEM((4, 256, 512), BF),
        pltpu.VMEM((4, 256, 512), BF),
        pltpu.VMEM((2, 2, 256, 128), BF),
        pltpu.VMEM((2, 2, 256, 128), BF),
        pltpu.VMEM((2, 16, 2, 256), F32),
        pltpu.VMEM((ROWS, 256), BF),
        pltpu.VMEM((ROWS, 256), BF),
        pltpu.VMEM((ROWS, 128), BF),
        pltpu.VMEM((NY, NX, ROWS, 128), BF),
        pltpu.VMEM((4, ROWS, 256), BF),
        pltpu.VMEM((4, ROWS, 128), BF),
        pltpu.VMEM((2, 2, ROWS // 4, 128), BF),
        pltpu.VMEM((2, 3, ROWS // 2, 128), BF),
        pltpu.VMEM((ROWS, 128), BF),
        pltpu.VMEM((ROWS, 128), BF),
        pltpu.VMEM((128, 256), BF),
        dma((len(args),)),
        dma((len(SENT),)),
        dma((len(RECV),)),
    ]
    return pl.pallas_call(
        kernel,
        out_shape=jax.ShapeDtypeStruct((256, 128), BF),
        in_specs=[pl.BlockSpec(memory_space=pl.ANY)] * len(args),
        out_specs=pl.BlockSpec(memory_space=pltpu.VMEM),
        scratch_shapes=scratch,
        compiler_params=pltpu.CompilerParams(
            collective_id=0, has_side_effects=True, vmem_limit_bytes=48 * 1024 * 1024
        ),
    )(*args)


def solution(mesh):
    torus = Mesh(mesh.devices.reshape(NZ, NC, NY, NX), ("z", "c", "y", "x"))
    sp, tp = ("z", "c"), ("y", "x")
    in_specs = (
        P(sp, tp), P(sp, tp), P(sp, tp), P(None, tp), P(tp, None), P(sp, tp), P(sp), P(tp),
        P(tp), P(sp, None), P(sp, None), P(sp, None, tp), P(sp, None, tp), P(sp, None, tp),
    )
    return jax.shard_map(
        per_device, mesh=torus, in_specs=in_specs, out_specs=P(sp, tp), check_vma=False
    )
```

```python
import jax
import jax.numpy as jnp
from jax import lax
from jax.experimental import pallas as pl
from jax.experimental.pallas import tpu as pltpu
from jax.sharding import Mesh
from jax.sharding import PartitionSpec as P

D = 2048
CAP = 32
ALPHA = 8.0**0.25
EPSILON = 1e-05
LIMIT = 7.0
SLOPE = 1.702
MESH_ID = pl.DeviceIdType.MESH
BF = jnp.bfloat16
F32 = jnp.float32

NZ, NC, NY, NX = 16, 2, 4, 4
NSP = NZ * NC
ROWS = NSP * CAP
SIZES = (1, 2, 4, 4, 2, 2, 1)
GROUPS = len(SIZES)
STARTS = tuple(sum(SIZES[:g]) for g in range(GROUPS))
ORDER = tuple(range(16))
GATHER_DIRECT = (0,)
SUM_DIRECT = (5, 6)


def z_shift(k):
    step, side = k // 2, k % 2
    step = ORDER[step]
    if step == 0:
        return 0, side
    return ((step + 1) // 2 if step % 2 else NZ - step // 2), side


SCHEDULE = [
    ("a0", 1), ("a0", 0), ("a0", 2), ("a1", 1), ("a2", 0), ("a1", 2), ("a0", 4), ("a0", 3),
    ("a2", 2), ("a0", 5), ("a1", 4), ("a1", 3), ("a0", 6), ("a1", 5), ("a2", 4), ("a2", 3),
    ("a2", 1), ("a1", 6), ("a2", 5), ("a3", 2), ("a3", 4), ("c", 0), ("a2", 6), ("a3", 5),
    ("a3", 3), ("a3", 1), ("a3", 6), ("c", 4), ("c", 5), ("c", 3), ("h1", 4), ("c", 6), ("c", 2),
    ("h1", 3), ("d", 5), ("c", 1), ("d", 4), ("h1", 2), ("d", 6), ("h1", 0), ("d", 3), ("h1", 1),
    ("e2", 5), ("e1", 4), ("d", 2), ("d", 0), ("e2", 6), ("e1", 3), ("d", 1), ("e2", 4),
    ("e1", 2), ("e2", 3), ("e1", 0), ("e1", 1), ("e2", 2), ("e2", 0), ("e2", 1),
]


PEERS = sorted(
    range(1, NY * NX), key=lambda p: -min(p // NX, NY - p // NX) - min(p % NX, NX - p % NX)
)
NAMES = (
    ["halo", "ow", "co0", "co1", "st0", "st1", "ret"]
    + [f"down{h}{n}" for h in range(2) for n in range(3)]
    + [f"z{g}" for g in range(GROUPS)]
    + [f"{n}{g}" for g in range(GROUPS) for n in ("x0d", "x0r", "x1d", "x1r", "hd", "hr", "sd", "sr")]
)
RECV = {name: i for i, name in enumerate(NAMES)}
SENT_NAMES = ("halo", "ow", "co", "st0", "st1", "ret", "down0", "down1", "z", "x", "h", "s")
SENT = {name: i for i, name in enumerate(SENT_NAMES)}


def column_of(row_ref, size):
    eye = lax.broadcasted_iota(jnp.int32, (size, size), 0) == lax.broadcasted_iota(
        jnp.int32, (size, size), 1
    )
    row = jnp.broadcast_to(row_ref, (size, size))
    return jnp.sum(jnp.where(eye, row, 0.0), axis=1, keepdims=True)


def nt_dot(a, b, dims):
    return lax.dot_general(a, b, (dims, ((), ())), preferred_element_type=F32)


def kernel(*refs):
    away, out, near = refs[:14], refs[14], refs[15:29]
    og, ig, ci, taps, ow, res, doc, mg, fg, routes, rw, wg, wu, wdi = near
    (
        halo, co, wc, wda, wdb, wra, wrb, st, sp0, sp1, sb, x4, h4, p4, r1, r2, ob, ret, nrm,
        load_sems, sent_sems, recv_sems,
    ) = refs[29:]
    z, c = lax.axis_index("z"), lax.axis_index("c")
    y, x = lax.axis_index("y"), lax.axis_index("x")
    own = y * NX + x

    def send(src, dst, sent, recv, target):
        pltpu.make_async_remote_copy(
            src_ref=src,
            dst_ref=dst,
            send_sem=sent_sems.at[SENT[sent]],
            recv_sem=recv_sems.at[RECV[recv]],
            device_id=target,
            device_id_type=MESH_ID,
        ).start()

    def landed(like, recv):
        pltpu.make_async_remote_copy(
            src_ref=like,
            dst_ref=like,
            send_sem=sent_sems.at[0],
            recv_sem=recv_sems.at[RECV[recv]],
            device_id=(z, c, y, lax.rem(x + 1, NX)),
            device_id_type=MESH_ID,
        ).wait_recv()

    def drained(like, sent):
        pltpu.make_async_remote_copy(
            src_ref=like,
            dst_ref=like,
            send_sem=sent_sems.at[SENT[sent]],
            recv_sem=recv_sems.at[0],
            device_id=(z, c, y, lax.rem(x + 1, NX)),
            device_id_type=MESH_ID,
        ).wait_send()

    def in_plane(p):
        return lax.rem(y + p // NX, NY), lax.rem(x + p % NX, NX)

    def from_plane(p):
        return lax.rem(y + NY - p // NX, NY), lax.rem(x + NX - p % NX, NX)

    def along_z(k):
        dz, dc = z_shift(k)
        return (lax.rem(z + dz, NZ), lax.rem(c + dc, NC), y, x)

    def back_z(k):
        dz, dc = z_shift(k)
        return (lax.rem(z + NZ - dz, NZ), lax.rem(c + NC - dc, NC), y, x)

    barrier = pltpu.get_barrier_semaphore()
    loads = [
        pltpu.make_async_copy(far, here, load_sems.at[i])
        for i, (far, here) in enumerate(zip(away, near))
    ]
    for i in (1, 2, 6, 3, 0):
        loads[i].start()
    with jax.named_scope("signals"):
        for p in PEERS:
            py, px = in_plane(p)
            pl.semaphore_signal(barrier, inc=1, device_id=(z, c, py, px), device_id_type=MESH_ID)
        for k in range(NSP - 1, 0, -1):
            pl.semaphore_signal(barrier, inc=1, device_id=along_z(k), device_id_type=MESH_ID)

    for i in (4, 9, 5, 7, 8, 10, 13, 11, 12):
        loads[i].start()

    with jax.named_scope("local"):
        for i in (1, 2, 6, 3, 0):
            loads[i].wait()
        product = ig[...].astype(F32) * ci[...].astype(F32)
        marks = doc[...].astype(F32)
        halo[0, 0:32, :] = product[:, 128:256]
        halo[0, 32:40, :] = jnp.broadcast_to(marks[:, 128:256], (8, 128))
        tap = [column_of(taps[i : i + 1, :], 32) for i in range(3)]

    with jax.named_scope("entry"):
        pl.semaphore_wait(barrier, NY * NX - 1 + NSP - 1)

    my_rows = pl.ds(pl.multiple_of(own * 32, 32), 32)

    def mix(before, before_mark, piece, mark):
        lanes = lax.broadcasted_iota(jnp.int32, (32, 128), 1)
        lane_row = lax.broadcasted_iota(jnp.int32, (1, 128), 1)
        mixed = tap[2] * piece
        for shift in (1, 2):
            back = jnp.where(
                lanes < shift, pltpu.roll(before, shift, 1), pltpu.roll(piece, shift, 1)
            )
            back_mark = jnp.where(
                lane_row < shift, pltpu.roll(before_mark, shift, 1), pltpu.roll(mark, shift, 1)
            )
            same = jnp.where(back_mark == mark, 1.0, 0.0)
            mixed = mixed + (same * tap[2 - shift]) * back
        return mixed

    def send_mixed(part):
        cols = pl.ds(part * 128, 128)
        for p in PEERS:
            py, px = in_plane(p)
            send(co.at[my_rows, cols], co.at[my_rows, cols], "co", f"co{part}", (z, c, py, px))

    with jax.named_scope("halo_send"):
        send(halo.at[0], halo.at[1], "halo", "halo", (lax.rem(z + c, NZ), 1 - c, y, x))
        late = mix(product[:, 0:128], marks[:, 0:128], product[:, 128:256], marks[:, 128:256])
        co[my_rows, 128:256] = (og[:, 128:256].astype(F32) * late).astype(BF)
        send_mixed(1)
        loads[4].wait()
        for p in PEERS:
            py, px = in_plane(p)
            there = py * NX + px
            send(
                ow.at[:, pl.ds(pl.multiple_of(there * 128, 128), 128)], wc.at[my_rows, :],
                "ow", "ow", (z, c, py, px),
            )
        wc[my_rows, :] = ow[:, pl.ds(pl.multiple_of(own * 128, 128), 128)]
    with jax.named_scope("halo_wait"):
        landed(halo.at[1], "halo")
    with jax.named_scope("conv"):
        first = jnp.where((z == 0) & (c == 0), 1.0, 0.0)
        prior_mark = halo[1, 32:33, :] * (1.0 - first) - first
        early = mix(halo[1, 0:32, :], prior_mark, product[:, 0:128], marks[:, 0:128])
        co[my_rows, 0:128] = (og[:, 0:128].astype(F32) * early).astype(BF)
        send_mixed(0)
    with jax.named_scope("slots"):
        for i in (5, 7, 8, 9, 10):
            loads[i].wait()
        ids = lax.broadcasted_iota(jnp.int32, (NSP, 256), 0)
        hits = [(routes[i : i + 1, :] == ids).astype(F32) for i in range(2)]
        before = (
            lax.broadcasted_iota(jnp.int32, (256, 256), 0)
            < lax.broadcasted_iota(jnp.int32, (256, 256), 1)
        ).astype(F32)
        counts = jnp.dot(
            (hits[0] + hits[1]).astype(BF), before.astype(BF), preferred_element_type=F32
        )
        slots = lax.broadcasted_iota(jnp.int32, (ROWS, 256), 0)
        for i, chosen in ((0, sp0), (1, sp1)):
            rank = jnp.sum(hits[i] * counts, axis=0, keepdims=True).astype(jnp.int32)
            expert = routes[i : i + 1, :]
            ez = jnp.right_shift(expert, 1)
            ec = expert - 2 * ez
            dz = ez - z
            dz = jnp.where(dz < 0, dz + NZ, dz)
            dc = jnp.where(ec == c, 0, 1)
            step = jnp.where(dz == 0, 0, jnp.where(dz <= NZ // 2, 2 * dz - 1, 2 * (NZ - dz)))
            place = jnp.zeros_like(step)
            for here, there in enumerate(ORDER):
                place = jnp.where(step == there, here, place)
            step = place
            slot = (step * 2 + dc) * CAP + rank
            chosen[...] = jnp.where(slots == slot, 1.0, 0.0).astype(BF)
    with jax.named_scope("residual"):
        stream_t = ALPHA * res[...].astype(F32).T

    def ring(axis, step):
        if axis == "x":
            return (z, c, y, lax.rem(x + step + NX, NX))
        return (z, c, lax.rem(y + step + NY, NY), x)

    def spot(axis, step):
        return lax.rem((x if axis == "x" else y) + step + 4, 4)

    def down_rows(half, step, part=None):
        lead = spot("yx"[half], step)
        if half == 0:
            return wdi.at[lead] if part is None else wdi.at[lead, pl.ds(2 * part, 2)]
        return wdi.at[:, lead] if part is None else wdi.at[pl.ds(2 * part, 2), lead]

    def down_cols(half, step, part=None):
        cols = pl.ds(pl.multiple_of(spot("yx"[half], step) * 128, 128), 128)
        buf = (wda, wdb)[half]
        return buf.at[:, :, cols] if part is None else buf.at[pl.ds(2 * part, 2), :, cols]

    def down_sends():
        loads[13].wait()
        for half in range(2):
            for way in range(2):
                send(
                    down_rows(half, 2, way), (wra, wrb)[half].at[way], f"down{half}",
                    f"down{half}0", ring("yx"[half], 1 - 2 * way),
                )
        for half in range(2):
            for way in range(2):
                step = 1 - 2 * way
                send(
                    down_rows(half, step), down_cols(half, 0), f"down{half}", f"down{half}1",
                    ring("yx"[half], step),
                )
        own_y = pl.ds(pl.multiple_of(y * 128, 128), 128)
        own_x = pl.ds(pl.multiple_of(x * 128, 128), 128)
        wda[:, :, own_y] = wdi[y]
        wdb[:, :, own_x] = wdi[:, x]

    def down_relay():
        for half in range(2):
            landed((wra, wrb)[half], f"down{half}0")
            for way in range(2):
                step = 1 - 2 * way
                send(
                    (wra, wrb)[half].at[way], down_cols(half, -step, way), f"down{half}",
                    f"down{half}2", ring("yx"[half], step),
                )

    def down_end():
        for half in range(2):
            buf = (wda, wdb)[half]
            landed(buf.at[:, :, pl.ds(0, 256)], f"down{half}1")
            landed(buf.at[:, :, pl.ds(0, 128)], f"down{half}2")

    with jax.named_scope("mix_wait"):
        landed(wc.at[pl.ds(0, 480), :], "ow")
        landed(co.at[pl.ds(0, 480), pl.ds(0, 128)], "co1")
        landed(co.at[pl.ds(0, 480), pl.ds(0, 128)], "co0")
    with jax.named_scope("mix_dot"):
        stream_t = stream_t + nt_dot(wc[...], co[...], ((0,), (0,)))

    def norm(stream, which, gain_col):
        s1 = jnp.sum(stream, axis=0, keepdims=True)
        s2 = jnp.sum(stream * stream, axis=0, keepdims=True)
        sub = lax.broadcasted_iota(jnp.int32, (2, 256), 0)
        st[which, own] = jnp.where(sub == 0, s1, s2)
        for p in PEERS:
            py, px = in_plane(p)
            send(st.at[which, own], st.at[which, own], f"st{which}", f"st{which}", (z, c, py, px))
        if which == 0:
            down_sends()
        landed(st.at[which, pl.ds(0, 15)], f"st{which}")
        total = st[which, 0]
        for j in range(1, NY * NX):
            total = total + st[which, j]
        mean = total[0:1, :] / D
        spread = total[1:2, :] / D - mean * mean
        return (stream - mean) * lax.rsqrt(spread + EPSILON) * gain_col

    with jax.named_scope("norm_a"):
        normed_t = norm(stream_t, 0, column_of(mg[...], 128)).astype(BF)
    nrm[...] = normed_t

    def rows_of(g):
        return pl.ds(STARTS[g] * 64, SIZES[g] * 64)

    def ks_of(g):
        return range(STARTS[g] * 2, (STARTS[g] + SIZES[g]) * 2)

    with jax.named_scope("dispatch"):
        for g in range(GROUPS):
            rows = rows_of(g)
            chosen = sp0[rows, :] + sp1[rows, :]
            sb[rows, :] = nt_dot(chosen, normed_t, ((1,), (1,))).astype(BF)
            for k in ks_of(g):
                cut = pl.ds(k * CAP, CAP)
                if k == 0:
                    x4[y, x, cut, :] = sb[cut, :]
                else:
                    send(sb.at[cut, :], x4.at[y, x, cut, :], "z", f"z{g}", along_z(k))
    with jax.named_scope("down_relay"):
        down_relay()

    def span(g, half, part):
        length = SIZES[g] * 32
        start = STARTS[g] * 64 + half * length
        if part == "lo":
            return pl.ds(start, length // 2)
        if part == "hi":
            return pl.ds(start + length // 2, length // 2)
        return pl.ds(start, length)

    def slab(buf, g, half, phase, step, part=None):
        rows = span(g, half, part)
        if half == 0:
            if phase == 0:
                return buf.at[y, spot("x", step), rows, :]
            return buf.at[spot("y", step), :, rows, :]
        if phase == 0:
            return buf.at[spot("y", step), x, rows, :]
        return buf.at[:, spot("x", step), rows, :]

    def axis_of(half, phase):
        return "xy"[(half + phase) % 2]

    def steps_of(g, chosen):
        return (1, -1, 2) if g in chosen else (1, -1)

    def ag_like(g, phase, count):
        if phase == 0:
            return x4.at[0, pl.ds(0, count), rows_of(g), :]
        return x4.at[pl.ds(0, count), :, rows_of(g), :]

    def ag_send(g):
        for half in range(2):
            for step in steps_of(g, GATHER_DIRECT):
                mine = slab(x4, g, half, 0, 0)
                send(mine, mine, "x", f"x0d{g}", ring(axis_of(half, 0), step))

    def ag_onward(g, places):
        for place in places:
            for half in range(2):
                for step in steps_of(g, GATHER_DIRECT):
                    piece = slab(x4, g, half, 0, place)
                    send(piece, piece, "x", f"x1d{g}", ring(axis_of(half, 1), step))

    def ag_relay(g, phase):
        landed(ag_like(g, phase, 2), f"x{phase}d{g}")
        for half in range(2):
            for step, part in ((1, "lo"), (-1, "hi")):
                piece = slab(x4, g, half, phase, -step, part)
                send(
                    piece, piece, "x", f"x{phase}r{g}", ring(axis_of(half, phase), step)
                )

    def ag_end(g, phase):
        if g in GATHER_DIRECT:
            landed(ag_like(g, phase, 3), f"x{phase}d{g}")
        else:
            landed(ag_like(g, phase, 1), f"x{phase}r{g}")

    def expert_in(g):
        rows = rows_of(g)
        inputs = jnp.concatenate(
            [x4[b, a, rows, :] for b in range(NY) for a in range(NX)], axis=1
        )
        gate = jnp.minimum(jnp.dot(inputs, wg[...], preferred_element_type=F32), LIMIT)
        up = jnp.clip(jnp.dot(inputs, wu[...], preferred_element_type=F32), -LIMIT, LIMIT)
        hidden = ((up + 1.0) * gate * jax.nn.sigmoid(SLOPE * gate)).astype(BF)
        for half in range(2):
            h4[spot("xy"[half], 0), span(g, half, None), :] = hidden[
                half * SIZES[g] * 32 : (half + 1) * SIZES[g] * 32, :
            ]

    def hidden_at(g, half, step, part=None):
        return h4.at[spot("xy"[half], step), span(g, half, part), :]

    def hidden_send(g):
        for half in range(2):
            for step in steps_of(g, SUM_DIRECT):
                mine = hidden_at(g, half, 0)
                send(mine, mine, "h", f"hd{g}", ring("xy"[half], step))

    def hidden_relay(g):
        landed(h4.at[pl.ds(0, 2), rows_of(g), :], f"hd{g}")
        for half in range(2):
            for step, part in ((1, "lo"), (-1, "hi")):
                piece = hidden_at(g, half, -step, part)
                send(piece, piece, "h", f"hr{g}", ring("xy"[half], step))

    def hidden_end(g):
        if g in SUM_DIRECT:
            landed(h4.at[pl.ds(0, 3), rows_of(g), :], f"hd{g}")
        else:
            landed(h4.at[pl.ds(0, 1), rows_of(g), :], f"hr{g}")

    def expert_out(g):
        for half in range(2):
            rows = span(g, half, None)
            inputs = jnp.concatenate([h4[b, rows, :] for b in range(4)], axis=1)
            weights = (wda, wdb)[half][...].reshape(1024, 512)
            part = jnp.dot(inputs, weights, preferred_element_type=F32).astype(BF)
            for b in range(4):
                p4[b, rows, :] = part[:, b * 128 : (b + 1) * 128]

    def part_at(g, half, step, part=None):
        return p4.at[spot("yx"[half], step), span(g, half, part), :]

    def first_at(g, half, way):
        return r1.at[half, way, pl.ds(STARTS[g] * 16, SIZES[g] * 16), :]

    def second_at(g, half, way):
        return r2.at[half, way, pl.ds(STARTS[g] * 32, SIZES[g] * 32), :]

    def sum_first(g):
        for half in range(2):
            axis = "yx"[half]
            if g in SUM_DIRECT:
                for way, step in enumerate(steps_of(g, SUM_DIRECT)):
                    send(
                        part_at(g, half, step), second_at(g, half, way), "s", f"sd{g}",
                        ring(axis, step),
                    )
            else:
                for way, part in ((0, "lo"), (1, "hi")):
                    send(
                        part_at(g, half, 2, part), first_at(g, half, way), "s", f"sr{g}",
                        ring(axis, 1 - 2 * way),
                    )

    def sum_second(g):
        landed(p4.at[pl.ds(0, 1), rows_of(g), :], f"sr{g}")
        for half in range(2):
            for way, part in ((0, "lo"), (1, "hi")):
                step = 1 - 2 * way
                edge = part_at(g, half, step, part)
                came = first_at(g, half, way)
                edge[...] = (edge[...].astype(F32) + came[...].astype(F32)).astype(BF)
                send(
                    part_at(g, half, step), second_at(g, half, way), "s", f"sd{g}",
                    ring("yx"[half], step),
                )

    def sum_end(g):
        ways = len(steps_of(g, SUM_DIRECT))
        landed(p4.at[pl.ds(0, ways), rows_of(g), :], f"sd{g}")
        for half in range(2):
            total = part_at(g, half, 0)[...].astype(F32)
            for way in range(ways):
                total = total + second_at(g, half, way)[...].astype(F32)
            ob[span(g, half, None), :] = total.astype(BF)

    first_of = {stage: g for stage, g in reversed(SCHEDULE)}
    for stage, g in SCHEDULE:
        with jax.named_scope(f"{stage}_{g}"):
            if stage == "a0":
                skip = CAP if g == 0 else 0
                arrived = pl.ds(STARTS[g] * 64 + skip, SIZES[g] * 64 - skip)
                landed(x4.at[y, x, arrived, :], f"z{g}")
                ag_send(g)
                ag_onward(g, (0,))
            elif stage == "a1":
                ag_relay(g, 0)
                ag_onward(g, (-1, 1))
            elif stage == "a2":
                ag_end(g, 0)
                ag_onward(g, (-1, 1, 2) if g in GATHER_DIRECT else (2,))
            elif stage == "a3":
                ag_relay(g, 1)
            elif stage == "c":
                ag_end(g, 1)
                if g == first_of["c"]:
                    loads[11].wait()
                    loads[12].wait()
                expert_in(g)
                hidden_send(g)
            elif stage == "h1":
                hidden_relay(g)
            elif stage == "d":
                hidden_end(g)
                if g == first_of["d"]:
                    down_end()
                expert_out(g)
                sum_first(g)
            elif stage == "e1":
                sum_second(g)
            else:
                sum_end(g)
                for k in reversed(ks_of(g)):
                    cut = pl.ds(k * CAP, CAP)
                    if k == 0:
                        ret[cut, :] = ob[cut, :]
                    else:
                        send(ob.at[cut, :], ret.at[cut, :], "ret", "ret", back_z(k))

    with jax.named_scope("drain"):
        drained(halo.at[0], "halo")
        drained(wc.at[pl.ds(0, 480), :], "ow")
        drained(co.at[pl.ds(0, 480), :], "co")
        drained(st.at[0, pl.ds(0, 15)], "st0")
        drained(wda, "down0")
        drained(wdb, "down1")
        drained(sb.at[pl.ds(CAP, ROWS - CAP), :], "z")
        drained(x4.at[:, :, pl.ds(0, ROWS // 16 * 15), :], "x")
        drained(h4.at[pl.ds(0, 3)], "h")
        drained(p4.at[pl.ds(0, 3)], "s")
    with jax.named_scope("ret_wait"):
        landed(ret.at[pl.ds(CAP, ROWS - CAP), :], "ret")
    with jax.named_scope("combine"):
        results = ret[...]
        ffn = rw[0:1, :] * nt_dot(results, sp0[...], ((0,), (0,)))
        ffn = ffn + rw[1:2, :] * nt_dot(results, sp1[...], ((0,), (0,)))
        second = ALPHA * nrm[...].astype(F32) + ffn
    with jax.named_scope("norm_b"):
        out[...] = norm(second, 1, column_of(fg[...], 128)).T.astype(BF)
    drained(st.at[1, pl.ds(0, 15)], "st1")
    drained(ob.at[pl.ds(CAP, ROWS - CAP), :], "ret")


def per_device(
    out_gate, in_gate, conv_input, conv_taps, out_weight, residual, document, mix_gain,
    ffn_gain, routes, route_weight, expert_gate, expert_up, expert_down,
):
    args = (
        out_gate.T, in_gate.T, conv_input.T, conv_taps, out_weight, residual,
        document[None, :], mix_gain[None, :], ffn_gain[None, :], routes.T, route_weight.T,
        expert_gate[0], expert_up[0], expert_down[0].reshape(NY, NX, 256, 128),
    )
    args = tuple(pltpu.with_memory_space_constraint(arg, pltpu.HBM) for arg in args)
    dma = pltpu.SemaphoreType.DMA
    scratch = [pltpu.VMEM(arg.shape, arg.dtype) for arg in args] + [
        pltpu.VMEM((2, 40, 128), F32),
        pltpu.VMEM((512, 256), BF),
        pltpu.VMEM((512, 128), BF),
        pltpu.VMEM((4, 256, 512), BF),
        pltpu.VMEM((4, 256, 512), BF),
        pltpu.VMEM((2, 2, 256, 128), BF),
        pltpu.VMEM((2, 2, 256, 128), BF),
        pltpu.VMEM((2, 16, 2, 256), F32),
        pltpu.VMEM((ROWS, 256), BF),
        pltpu.VMEM((ROWS, 256), BF),
        pltpu.VMEM((ROWS, 128), BF),
        pltpu.VMEM((NY, NX, ROWS, 128), BF),
        pltpu.VMEM((4, ROWS, 256), BF),
        pltpu.VMEM((4, ROWS, 128), BF),
        pltpu.VMEM((2, 2, ROWS // 4, 128), BF),
        pltpu.VMEM((2, 3, ROWS // 2, 128), BF),
        pltpu.VMEM((ROWS, 128), BF),
        pltpu.VMEM((ROWS, 128), BF),
        pltpu.VMEM((128, 256), BF),
        dma((len(args),)),
        dma((len(SENT),)),
        dma((len(RECV),)),
    ]
    return pl.pallas_call(
        kernel,
        out_shape=jax.ShapeDtypeStruct((256, 128), BF),
        in_specs=[pl.BlockSpec(memory_space=pl.ANY)] * len(args),
        out_specs=pl.BlockSpec(memory_space=pltpu.VMEM),
        scratch_shapes=scratch,
        compiler_params=pltpu.CompilerParams(
            collective_id=0, has_side_effects=True, vmem_limit_bytes=48 * 1024 * 1024
        ),
    )(*args)


def solution(mesh):
    torus = Mesh(mesh.devices.reshape(NZ, NC, NY, NX), ("z", "c", "y", "x"))
    sp, tp = ("z", "c"), ("y", "x")
    in_specs = (
        P(sp, tp), P(sp, tp), P(sp, tp), P(None, tp), P(tp, None), P(sp, tp), P(sp), P(tp),
        P(tp), P(sp, None), P(sp, None), P(sp, None, tp), P(sp, None, tp), P(sp, None, tp),
    )
    return jax.shard_map(
        per_device, mesh=torus, in_specs=in_specs, out_specs=P(sp, tp), check_vma=False
    )
```
